256 devices in a mesh: sp: 32 (over z, y), tp: 8 (over x, core).
Axes of the slice: x: 4, y: 4, z: 8, core: 2. Of those that a mesh axis runs over, the one named last changes fastest.
Arguments:
- residual_in: bfloat16 [12288, 2048], P(('sp', 'tp')), may hold values from -6 to 6
- queries: bfloat16 [12288, 2048], P('sp', 'tp'), may hold values from -180 to 180
- keys: bfloat16 [12288, 2048], P('sp', 'tp'), may hold values from -9 to 9
- values: bfloat16 [12288, 2048], P('sp', 'tp'), may hold values from -6 to 6
- mix_lambda: float32 [16], P('tp'), may hold values from 0.3 to 0.8
- head_gain: float32 [128], replicated, may hold values from 0.1 to 1.9
- out_weight: bfloat16 [2048, 2048], P('tp'), may hold values from -0.125 to 0.125
- norm_gain: float32 [2048], replicated, may hold values from 0.1 to 1.9
- gate_weight: bfloat16 [2048, 5632], P('sp', 'tp'), may hold values from -0.125 to 0.125
- up_weight: bfloat16 [2048, 5632], P('sp', 'tp'), may hold values from -0.125 to 0.125
- down_weight: bfloat16 [5632, 2048], P('tp', 'sp'), may hold values from -0.078125 to 0.078125
Outputs:
- layer_out: bfloat16 [12288, 2048], P(('sp', 'tp'))
The draws below stay inside these ranges and needn't reach their ends.
All inputs are finite; a program needn't handle non-finite values.
Results may differ from the reference program's by a relative error of at most 0.014.
Values may be sent and summed in bfloat16 or wider, within the bound.
No kernel may reach another device: no remote copies, remote signals or barrier semaphores. Data moves between devices by JAX's collectives and lax.ppermute only.
A program may use at most 128 MiB of HBM per device.

```python
import math
import jax
import jax.numpy as jnp
from jax import lax

D = 2048
H = 16
DH = 64
VD = 128
FF = 5632
TOKENS = 12288


def shared_keys(key):
    base = jax.random.fold_in(key, 101)
    drawn = jnp.clip(1.3 * jax.random.normal(jax.random.fold_in(base, 1), (TOKENS, H * 2 * DH), jnp.float32), -8.0, 8.0)
    return drawn


def draw_keys(key, part):
    drawn = shared_keys(key)
    return drawn.astype(jnp.bfloat16)


def draw_queries(key, part):
    base = jax.random.fold_in(key, 202)
    drawn = jnp.clip(1.3 * jax.random.normal(jax.random.fold_in(base, 1), (TOKENS, H * 2 * DH), jnp.float32), -8.0, 8.0)
    return drawn.astype(jnp.bfloat16)


def block_levels(own_key, dims, shards, low, largest):
    loudness, own = 1.0, jax.random.fold_in(own_key, 6)
    for position, parts in shards:
        heights = jnp.exp(jax.random.uniform(jax.random.fold_in(own, position), (parts,), jnp.float32, low / len(shards), largest / len(shards)))
        loudness = loudness * jnp.repeat(heights, dims[position] // parts).reshape([-1 if axis == position else 1 for axis in range(len(dims))])
    return loudness


def bell_draw(key, extent, width, limit, cuts=(), kind=jnp.bfloat16):
    values = jax.random.normal(key, extent, jnp.float32) * width
    if len(cuts) > 0:
        values = block_levels(key, extent, cuts, -0.22, 0.18) * values
    return jnp.clip(values, min=-limit, max=limit).astype(kind)


def setup_inputs(seed: int = 0) -> dict:
    arg_keys = jax.random.split(jax.random.key(seed), 12)
    return {
        "residual_in": bell_draw(arg_keys[0], (TOKENS, D), 1.0, 6.0, ((0, 256),)),
        "queries": draw_queries(jax.random.fold_in(arg_keys[11], 71), 0),
        "keys": draw_keys(jax.random.fold_in(arg_keys[11], 71), 0),
        "values": bell_draw(arg_keys[3], (TOKENS, H * VD), 1.0, 6.0, ((0, 32), (1, 8))),
        "mix_lambda": jnp.clip(0.3 + 0.5 * jax.random.uniform(arg_keys[4], (H,), jnp.float32) ** block_levels(arg_keys[4], (H,), ((0, 8),), -0.2, 0.2), 0.3, 0.8),
        "head_gain": jnp.clip(1.0 + 0.18 * jax.random.normal(arg_keys[5], (VD,), jnp.float32), 0.1, 1.9),
        "out_weight": bell_draw(arg_keys[6], (H * VD, D), (H * VD) ** -0.5, 0.125, ((0, 8),)),
        "norm_gain": jnp.clip(1.0 + 0.18 * jax.random.normal(arg_keys[7], (D,), jnp.float32), 0.1, 1.9),
        "gate_weight": bell_draw(arg_keys[8], (D, FF), D ** -0.5, 0.125, ((0, 32), (1, 8))),
        "up_weight": bell_draw(arg_keys[9], (D, FF), D ** -0.5, 0.125, ((0, 32), (1, 8))),
        "down_weight": bell_draw(arg_keys[10], (FF, D), FF ** -0.5, 0.078125, ((0, 8), (1, 32))),
    }


def head_rows(args):
    query_head, key_head, value_head, weight_two, head_gain = args
    block_rows = math.gcd(512, TOKENS)
    blocks = query_head.reshape(TOKENS // block_rows, block_rows, 2, DH)
    key_float = key_head.astype(jnp.float32)
    value_float = value_head.astype(jnp.float32)

    def one_block(query_block):
        scores = jnp.einsum('qcd,kcd->cqk', query_block.astype(jnp.float32), key_float) / math.sqrt(DH)
        top = lax.optimization_barrier(jnp.max(scores, axis=-1, keepdims=True))
        expo = jnp.exp(scores - top)
        total = lax.optimization_barrier(jnp.sum(expo, axis=-1, keepdims=True))
        probs = lax.optimization_barrier(expo.astype(jnp.bfloat16)).astype(jnp.float32)
        maps = jnp.einsum('cqk,ke->cqe', probs, value_float) / total
        mixed = maps[0] - weight_two * maps[1]
        scale = lax.rsqrt(lax.optimization_barrier(jnp.mean(mixed * mixed, axis=-1, keepdims=True)) + 1e-06)
        return (mixed * scale * head_gain).astype(jnp.bfloat16)
    return lax.map(one_block, blocks).reshape(TOKENS, VD)

def reference(residual_in, queries, keys, values, mix_lambda, head_gain, out_weight, norm_gain, gate_weight, up_weight, down_weight):
    query_heads = jnp.transpose(queries.reshape(TOKENS, H, 2, DH), (1, 0, 2, 3))
    key_heads = jnp.transpose(keys.reshape(TOKENS, H, 2, DH), (1, 0, 2, 3))
    value_heads = jnp.transpose(values.reshape(TOKENS, H, VD), (1, 0, 2))
    gains = jnp.broadcast_to(head_gain, (H, VD))
    per_head = lax.map(head_rows, (query_heads, key_heads, value_heads, mix_lambda, gains))
    attended = jnp.transpose(per_head, (1, 0, 2)).reshape(TOKENS, H * VD)
    after_mix = residual_in.astype(jnp.float32) + jnp.dot(attended, out_weight, preferred_element_type=jnp.float32)
    scale = lax.rsqrt(lax.optimization_barrier(jnp.mean(after_mix * after_mix, axis=-1, keepdims=True)) + 1e-06)
    normed = (after_mix * scale * norm_gain).astype(jnp.bfloat16)
    gate = jnp.dot(normed, gate_weight, preferred_element_type=jnp.float32)
    up = jnp.dot(normed, up_weight, preferred_element_type=jnp.float32)
    hidden = (jax.nn.silu(gate) * up).astype(jnp.bfloat16)
    mixer = jnp.dot(hidden, down_weight, preferred_element_type=jnp.float32)
    return (after_mix + 0.5 * mixer).astype(jnp.bfloat16)
```

```python
import functools

import jax
import jax.numpy as jnp
from jax import lax
from jax.experimental import pallas as pl
from jax.experimental.pallas import tpu as pltpu
from jax.sharding import Mesh, PartitionSpec as P

BF = jnp.bfloat16
F32 = jnp.float32
Z, Y, X, C = 8, 4, 4, 2
TQ = 256


def whole(n):
    return [pl.BlockSpec(memory_space=pltpu.VMEM)] * n


def attend_body(*refs, pieces, first):
    count = 1 + max(p[0] for p in pieces)
    q_ref, kv_refs = refs[0], refs[1 : 1 + count]
    old_ref = None if first else refs[1 + count]
    new_ref, sa, sb = refs[-3:]
    tiles = q_ref.shape[0] // TQ
    keys = 384 * len(pieces)

    def scores(t, s):
        q = q_ref[pl.ds(pl.multiple_of(t * TQ, TQ), TQ), :]
        top = None
        for j, (which, row, _) in enumerate(pieces):
            d = lax.dot_general(
                kv_refs[which][row : row + 384, :], q, (((1,), (1,)), ((), ())), preferred_element_type=F32
            )
            s[384 * j : 384 * (j + 1), :] = d
            m = jnp.max(d.reshape(48, 8, TQ), axis=0)
            top = m if top is None else jnp.maximum(top, m)
        return jnp.max(top, axis=0, keepdims=True)

    def add(t, s, top):
        at = pl.ds(pl.multiple_of(t * TQ, TQ), TQ)
        if not first:
            old_top = old_ref[136:137, at]
            top = jnp.maximum(old_top, top)
        total = None
        for j in range(0, len(pieces), 2):
            p = jnp.exp(s[384 * j : 384 * (j + 2), :] - top).astype(BF)
            v = jnp.concatenate(
                [kv_refs[w][row + 128 * i : row + 128 * (i + 1), :] for w, _, row in pieces[j : j + 2] for i in range(3)],
                axis=1,
            )
            ones = jnp.ones((16, 768), BF)
            d = jnp.dot(jnp.concatenate([v, ones], axis=0), p, preferred_element_type=F32)
            total = d if total is None else total + d
        total = total[:136]
        if not first:
            total = old_ref[0:136, at] * jnp.exp(old_top - top) + total
        new_ref[0:136, at] = total
        new_ref[136:144, at] = jnp.broadcast_to(top, (8, TQ))

    def body(i, top):
        t = 2 * i
        top_b = scores(t + 1, sb)
        add(t, sa, top)
        top_a = scores(jnp.minimum(t + 2, tiles - 1), sa)
        add(t + 1, sb, top_b)
        return top_a

    lax.fori_loop(0, tiles // 2, body, scores(0, sa))


def attend(q, arrays, pieces, state):
    first = state is None
    n = q.shape[0]
    keys = 384 * len(pieces)
    out = jax.ShapeDtypeStruct((144, n), F32)
    args = [q, *arrays] + ([] if first else [state])
    return pl.pallas_call(
        functools.partial(attend_body, pieces=pieces, first=first),
        in_specs=whole(len(args)),
        out_specs=pl.BlockSpec(memory_space=pltpu.VMEM),
        out_shape=out,
        scratch_shapes=[pltpu.VMEM((keys, TQ), F32)] * 2,
        input_output_aliases={} if first else {len(args) - 1: 0},
        compiler_params=pltpu.CompilerParams(vmem_limit_bytes=20 * 2**20),
        cost_estimate=pl.CostEstimate(flops=8 * 256 * n * keys, bytes_accessed=2**22, transcendentals=n * keys),
        name="attend",
    )(*args)


def block_body(kv_ref, out_ref):
    for half in range(2):
        out_ref[768 * half : 768 * half + 384, :] = kv_ref[384 * half : 384 * (half + 1), 0:128]
        for i in range(3):
            row = 384 * half + 128 * i
            out_ref[768 * half + 384 + 128 * i : 768 * half + 512 + 128 * i, :] = kv_ref[row : row + 128, 128:256].T


def make_block(kv):
    return pl.pallas_call(
        block_body,
        in_specs=whole(1),
        out_specs=pl.BlockSpec(memory_space=pltpu.VMEM),
        out_shape=jax.ShapeDtypeStruct((1536, 128), BF),
        cost_estimate=pl.CostEstimate(flops=10**7, bytes_accessed=2**20, transcendentals=0),
        name="block",
    )(kv)


def finish_body(mine_ref, other_ref, lam_ref, gain_ref, out_ref):
    n = out_ref.shape[0]
    lam = lam_ref[0]
    gain = gain_ref[...]
    for t in range(n // 128):
        maps = []
        for comp in range(2):
            at = slice(n * comp + 128 * t, n * comp + 128 * (t + 1))
            m0, m1 = mine_ref[136:137, at], other_ref[136:137, at]
            top = jnp.maximum(m0, m1)
            w0, w1 = jnp.exp(m0 - top), jnp.exp(m1 - top)
            total = mine_ref[128:129, at] * w0 + other_ref[128:129, at] * w1
            maps.append((mine_ref[0:128, at] * w0 + other_ref[0:128, at] * w1) / total)
        mixed = maps[0] - lam * maps[1]
        scale = lax.rsqrt(jnp.mean(mixed * mixed, axis=0, keepdims=True) + 1e-06)
        out_ref[128 * t : 128 * (t + 1), :] = ((mixed * scale).T * gain).astype(BF)


def finish(mine, other, lam, gain):
    n = mine.shape[1] // 2
    return pl.pallas_call(
        finish_body,
        in_specs=[*whole(2), pl.BlockSpec(memory_space=pltpu.SMEM), *whole(1)],
        out_specs=pl.BlockSpec(memory_space=pltpu.VMEM),
        out_shape=jax.ShapeDtypeStruct((n, 128), BF),
        cost_estimate=pl.CostEstimate(flops=10**8, bytes_accessed=2**21, transcendentals=0),
        name="finish",
    )(mine, other, lam, gain)


def mixer_body(x_ref, w_ref, out_ref, gu, down, hid):
    k = pl.program_id(0)
    x = x_ref[:, pl.ds(pl.multiple_of(k * 256, 256), 256)]
    for c in range(2):
        d = jnp.dot(x, w_ref[:, c, :, 0:1408].reshape(256, 1408), preferred_element_type=F32)

        @pl.when(k == 0)
        def _():
            gu[c] = d

        @pl.when(k > 0)
        def _():
            gu[c] += d

        down[c, pl.ds(pl.multiple_of(k * 256, 256), 256), :] = w_ref[:, c, :, 1408:2176].reshape(256, 768)

    @pl.when(k == pl.num_programs(0) - 1)
    def _():
        for c in range(2):
            for a, b in ((0, 640), (128, 768), (256, 896), (384, 1024), (512, 1152)):
                hid[:, 768 * c + a : 768 * c + a + 128] = (
                    jax.nn.silu(gu[c, :, a : a + 128]) * gu[c, :, b : b + 128]
                ).astype(BF)
            tail = gu[c, :, 1280:1408]
            both = jax.nn.silu(tail) * pltpu.roll(tail, 64, 1)
            lane = lax.broadcasted_iota(jnp.int32, both.shape, 1)
            hid[:, 768 * c + 640 : 768 * c + 768] = jnp.where(lane < 64, both, 0.0).astype(BF)
        for n in range(8):
            rows = slice(256 * n, 256 * (n + 1))
            total = None
            for c in range(2):
                d = lax.dot_general(
                    hid[:, 768 * c : 768 * (c + 1)], down[c, rows, :], (((1,), (1,)), ((), ())), preferred_element_type=F32
                )
                total = d if total is None else total + d
            out_ref[:, rows] = total.astype(BF)


def mixer(x, w):
    rows = x.shape[0]
    return pl.pallas_call(
        mixer_body,
        grid=(8,),
        in_specs=[
            pl.BlockSpec((rows, 2048), lambda k: (0, 0)),
            pl.BlockSpec((4, 2, 64, 2176), lambda k: (k, 0, 0, 0)),
        ],
        out_specs=pl.BlockSpec((rows, 2048), lambda k: (0, 0)),
        out_shape=jax.ShapeDtypeStruct((rows, 2048), BF),
        scratch_shapes=[pltpu.VMEM((2, rows, 1408), F32), pltpu.VMEM((2, 2048, 768), BF), pltpu.VMEM((rows, 1536), BF)],
        compiler_params=pltpu.CompilerParams(vmem_limit_bytes=40 * 2**20),
        cost_estimate=pl.CostEstimate(flops=6 * rows * 2048 * 1408, bytes_accessed=18 * 2**20, transcendentals=0),
        name="mixer",
    )(x, w)


def swap(v):
    return lax.ppermute(v, "c", [(0, 1), (1, 0)])


def around(v, step):
    return lax.ppermute(v, "z", [(i, (i + step) % Z) for i in range(Z)])


def exchange(v, axis):
    return lax.all_to_all(v, axis, split_axis=0, concat_axis=0, tiled=True)


def body(residual, queries, keys, values, mix_lambda, head_gain, out_weight, norm_gain, gate, up, down):
    x, y, c = lax.axis_index("x"), lax.axis_index("y"), lax.axis_index("c")
    tokens = queries.shape[0]
    half = tokens // 2

    packed = jnp.concatenate(
        [gate[:, :640], up[:, :640], gate[:, 640:], up[:, 640:], down.T, jnp.zeros((64, 64), BF)], axis=1
    )
    weights = lax.all_gather(packed, ("z", "y", "c"), axis=0, tiled=False).reshape(32, 2, 64, 2176)

    kv = jnp.concatenate([keys, values], axis=1)
    mine = lax.dynamic_slice_in_dim(kv, c * half, half, 0)
    got = swap(lax.dynamic_slice_in_dim(kv, (1 - c) * half, half, 0))
    low, high = jnp.where(c == 0, mine, got), jnp.where(c == 0, got, mine)
    heads = [
        jnp.concatenate([d[:, 128 * j : 128 * (j + 1)], d[:, 256 + 128 * j : 256 + 128 * (j + 1)]], axis=1)
        for d in (low, high)
        for j in range(2)
    ]
    kv_head = exchange(jnp.stack(heads), "y").reshape(4 * half, 256)
    block = make_block(kv_head)
    right, left = around(block, 1), around(block, -1)

    q_got = swap(queries)
    low, high = jnp.where(c == 0, queries, q_got), jnp.where(c == 0, q_got, queries)
    q_head = exchange(jnp.stack([d[:, 128 * j : 128 * (j + 1)] for d in (low, high) for j in range(2)]), "y")
    q_head = q_head.reshape(Y, X, C, 48, 128) * BF(0.125)
    lane = lax.broadcasted_iota(jnp.int32, (1, 128), 1)
    q_cols = []
    for sub in range(2):
        part = q_head[:, :, sub].reshape(768, 128)
        q_cols += [jnp.where(lane < 64, part, BF(0)), jnp.where(lane < 64, BF(0), part)]
    q_all = jnp.concatenate(q_cols, axis=0)

    one = [(0, 0, 384), (0, 768, 1152)]
    two = one + [(1, 0, 384), (1, 768, 1152)]
    state = attend(q_all, [block], one, None)
    right2, left2 = around(right, 1), around(left, -1)
    state = attend(q_all, [right, left], two, state)
    right3, left3 = around(right2, 1), around(left2, -1)
    state = attend(q_all, [right2, left2], two, state)
    last_r, last_l = around(right3[:768], 1), around(left3[768:], -1)
    state = attend(q_all, [right3, left3], two, state)
    state = attend(q_all, [last_r, last_l], [(0, 0, 384), (1, 0, 384)], state)

    own = lax.dynamic_slice_in_dim(state, c * 1536, 1536, 1)
    other = swap(lax.dynamic_slice_in_dim(state, (1 - c) * 1536, 1536, 1))
    lam_got = swap(mix_lambda)
    lam4 = jnp.where(c == 0, jnp.concatenate([mix_lambda, lam_got]), jnp.concatenate([lam_got, mix_lambda]))
    lam = lax.dynamic_slice_in_dim(lam4, y, 1, 0)
    attended = finish(own, other, lam, head_gain.reshape(1, 128))

    heads = exchange(attended.reshape(Y, 192, 128), "y")
    w_got = swap(out_weight)
    a_mine = lax.dynamic_slice_in_dim(heads, 2 * c, 2, 0)
    a_other = lax.dynamic_slice_in_dim(heads, 2 - 2 * c, 2, 0)
    side = lambda a: jnp.concatenate([a[0], a[1]], axis=1)
    part = jnp.dot(side(a_mine), out_weight, preferred_element_type=F32) + jnp.dot(
        side(a_other), w_got, preferred_element_type=F32
    )
    projected = exchange(part.astype(BF).reshape(X, 48, 2048), "x").astype(F32).sum(axis=0)
    after_mix = residual.astype(F32) + projected
    scale = lax.rsqrt(jnp.mean(after_mix * after_mix, axis=-1, keepdims=True) + 1e-06)
    normed = (after_mix * scale * norm_gain).astype(BF)
    rows = exchange(jnp.broadcast_to(normed, (X, 48, 2048)), "x").reshape(192, 2048)
    mixed = exchange(mixer(rows, weights).reshape(X, 48, 2048), "x").astype(F32).sum(axis=0)
    return (after_mix + 0.5 * mixed).astype(BF)


def solution(mesh):
    split = Mesh(mesh.devices.reshape(Z, Y, X, C), ("z", "y", "x", "c"))
    sp, tp = ("z", "y"), ("x", "c")
    return jax.shard_map(
        body,
        mesh=split,
        in_specs=(
            P(("z", "y", "x", "c"), None),
            P(sp, tp),
            P(sp, tp),
            P(sp, tp),
            P(tp),
            P(),
            P(tp, None),
            P(),
            P(sp, tp),
            P(sp, tp),
            P(tp, sp),
        ),
        out_specs=P(("z", "y", "x", "c"), None),
        check_vma=False,
    )
```

```python
import functools

import jax
import jax.numpy as jnp
from jax import lax
from jax.experimental import pallas as pl
from jax.experimental.pallas import tpu as pltpu
from jax.sharding import Mesh, PartitionSpec as P

BF = jnp.bfloat16
F32 = jnp.float32
Z, Y, X, C = 8, 4, 4, 2
TQ = 256


def whole(n):
    return [pl.BlockSpec(memory_space=pltpu.VMEM)] * n


def attend_body(*refs, pieces, first, parts, start):
    count = 1 + max(p[0] for p in pieces)
    q_ref, kv_refs = refs[0], refs[1 : 1 + count]
    old_refs = [None] * parts if first else refs[1 + count : 1 + count + parts]
    new_refs = refs[-2 - parts : -2]
    sa, sb = refs[-2:]
    each = new_refs[0].shape[1] // TQ
    tiles = each * parts

    def scores(t, s):
        q = q_ref[pl.ds(pl.multiple_of((start + t) * TQ, TQ), TQ), :]
        top = None
        for j, (which, row, _) in enumerate(pieces):
            d = lax.dot_general(
                kv_refs[which][row : row + 384, :], q, (((1,), (1,)), ((), ())), preferred_element_type=F32
            )
            s[384 * j : 384 * (j + 1), :] = d
            m = jnp.max(d.reshape(48, 8, TQ), axis=0)
            top = m if top is None else jnp.maximum(top, m)
        return jnp.max(top, axis=0, keepdims=True)

    def add(t, s, top, old_ref, new_ref):
        at = pl.ds(pl.multiple_of(t * TQ, TQ), TQ)
        if not first:
            old_top = old_ref[136:137, at]
            top = jnp.maximum(old_top, top)
        total = None
        for j in range(0, len(pieces), 2):
            p = jnp.exp(s[384 * j : 384 * (j + 2), :] - top).astype(BF)
            v = jnp.concatenate(
                [kv_refs[w][row + 128 * i : row + 128 * (i + 1), :] for w, _, row in pieces[j : j + 2] for i in range(3)],
                axis=1,
            )
            ones = jnp.ones((16, 768), BF)
            d = jnp.dot(jnp.concatenate([v, ones], axis=0), p, preferred_element_type=F32)
            total = d if total is None else total + d
        total = total[:136]
        if not first:
            total = old_ref[0:136, at] * jnp.exp(old_top - top) + total
        new_ref[0:136, at] = total
        new_ref[136:144, at] = jnp.broadcast_to(top, (8, TQ))

    top = scores(0, sa)
    for part in range(parts):

        def body(i, top):
            t = 2 * i
            base = each * part
            top_b = scores(base + t + 1, sb)
            add(t, sa, top, old_refs[part], new_refs[part])
            top_a = scores(jnp.minimum(base + t + 2, tiles - 1), sa)
            add(t + 1, sb, top_b, old_refs[part], new_refs[part])
            return top_a

        top = lax.fori_loop(0, each // 2, body, top)


def attend(q, arrays, pieces, states, parts=2, start=0):
    first = states is None
    n = 1536 * parts
    keys = 384 * len(pieces)
    args = [q, *arrays] + ([] if first else list(states))
    return pl.pallas_call(
        functools.partial(attend_body, pieces=pieces, first=first, parts=parts, start=start),
        in_specs=whole(len(args)),
        out_specs=whole(parts),
        out_shape=[jax.ShapeDtypeStruct((144, n // parts), F32)] * parts,
        scratch_shapes=[pltpu.VMEM((keys, TQ), F32)] * 2,
        input_output_aliases={} if first else {len(args) - parts + i: i for i in range(parts)},
        compiler_params=pltpu.CompilerParams(vmem_limit_bytes=16 * 2**20),
        cost_estimate=pl.CostEstimate(flops=8 * 256 * n * keys, bytes_accessed=2**22, transcendentals=n * keys),
        name="attend",
    )(*args)


def pack_body(gate_ref, up_ref, down_ref, out_ref):
    out_ref[:, 0:640] = gate_ref[:, 0:640]
    out_ref[:, 640:1280] = up_ref[:, 0:640]
    tails = [r[:, 640:704].astype(F32) for r in (gate_ref, up_ref)]
    out_ref[:, 1280:1408] = jnp.concatenate(tails, axis=1).astype(BF)
    row, col = (lax.broadcasted_iota(jnp.int32, (64, 64), i) for i in range(2))
    eye = jnp.where(row == col, 1.0, 0.0).astype(BF)
    turned = lax.dot_general(eye, down_ref[...], (((1,), (1,)), ((), ())), preferred_element_type=F32).astype(BF)
    out_ref[:, 1408:2048] = turned[:, 0:640]
    last = jnp.concatenate([turned[:, 640:704].astype(F32), jnp.zeros((64, 64), F32)], axis=1)
    out_ref[:, 2048:2176] = last.astype(BF)


def small(body, name, shapes, scalars, *args):
    alone = not isinstance(shapes, list)
    return pl.pallas_call(
        body,
        in_specs=[pl.BlockSpec(memory_space=pltpu.SMEM)] * scalars + whole(len(args) - scalars),
        out_specs=pl.BlockSpec(memory_space=pltpu.VMEM) if alone else whole(len(shapes)),
        out_shape=jax.ShapeDtypeStruct(*shapes) if alone else [jax.ShapeDtypeStruct(*sh) for sh in shapes],
        compiler_params=pltpu.CompilerParams(vmem_limit_bytes=8 * 2**20),
        cost_estimate=pl.CostEstimate(flops=10**7, bytes_accessed=2**20, transcendentals=0),
        name=name,
    )(*args)


def send_body(c_ref, q_ref, k_ref, v_ref, out_ref):
    at = pl.ds(pl.multiple_of((1 - c_ref[0]) * 192, 192), 192)
    out_ref[0:384, :] = q_ref[...]
    out_ref[384:576, :] = k_ref[at, :]
    out_ref[576:768, :] = v_ref[at, :]


def heads_body(c_ref, q_ref, k_ref, v_ref, got_ref, out_ref):
    c = c_ref[0]
    at = pl.ds(pl.multiple_of(c * 192, 192), 192)
    for j in range(2):
        lanes = slice(128 * j, 128 * (j + 1))
        out_ref[2 * c + j, 0:384, :] = q_ref[:, lanes]
        out_ref[2 * c + j, 384:576, :] = k_ref[at, lanes]
        out_ref[2 * c + j, 576:768, :] = v_ref[at, lanes]
        out_ref[2 - 2 * c + j] = got_ref[:, lanes]


def block_body(head_ref, out_ref):
    for i in range(4):
        at = 768 * (i // 2) + 192 * (i % 2)
        out_ref[at : at + 192, :] = head_ref[i, 384:576, :]
    values = jnp.concatenate([head_ref[i, 576:768, :] for i in range(4)], axis=0)
    for i in range(6):
        at = 768 * (i // 3) + 384 + 128 * (i % 3)
        out_ref[at : at + 128, :] = values[128 * i : 128 * (i + 1), :].T


def queries_body(c_ref, head_ref, out_ref):
    c = c_ref[0]
    lane = lax.broadcasted_iota(jnp.int32, (48, 128), 1)
    for i in range(2):
        sub = 1 - c if i == 0 else c
        for y in range(4):
            for x in range(4):
                rows = head_ref[y, pl.ds(pl.multiple_of(96 * x + 48 * sub, 48), 48), :].astype(F32) * 0.125
                at = 1536 * i + 192 * y + 48 * x
                out_ref[at : at + 48, :] = jnp.where(lane < 64, rows, 0.0).astype(BF)
                out_ref[at + 768 : at + 816, :] = jnp.where(lane < 64, 0.0, rows).astype(BF)


def finish_body(mine_ref, other_ref, lam_ref, gain_ref, out_ref):
    n = out_ref.shape[0]
    lam = lam_ref[0]
    gain = gain_ref[...]
    for t in range(n // 128):
        maps = []
        for comp in range(2):
            at = slice(n * comp + 128 * t, n * comp + 128 * (t + 1))
            m0, m1 = mine_ref[136:137, at], other_ref[136:137, at]
            top = jnp.maximum(m0, m1)
            w0, w1 = jnp.exp(m0 - top), jnp.exp(m1 - top)
            total = mine_ref[128:129, at] * w0 + other_ref[128:129, at] * w1
            maps.append((mine_ref[0:128, at] * w0 + other_ref[0:128, at] * w1) / total)
        mixed = maps[0] - lam * maps[1]
        scale = lax.rsqrt(jnp.mean(mixed * mixed, axis=0, keepdims=True) + 1e-06)
        out_ref[128 * t : 128 * (t + 1), :] = ((mixed * scale).T * gain).astype(BF)


def finish(mine, other, lam, gain):
    n = mine.shape[1] // 2
    return pl.pallas_call(
        finish_body,
        in_specs=[*whole(2), pl.BlockSpec(memory_space=pltpu.SMEM), *whole(1)],
        out_specs=pl.BlockSpec(memory_space=pltpu.VMEM),
        out_shape=jax.ShapeDtypeStruct((n, 128), BF),
        compiler_params=pltpu.CompilerParams(vmem_limit_bytes=8 * 2**20),
        cost_estimate=pl.CostEstimate(flops=10**8, bytes_accessed=2**21, transcendentals=0),
        name="finish",
    )(mine, other, lam, gain)


def mixer_body(x_ref, w_hbm, out_ref, w_ref, gu, hid, sems):
    parts = sems.shape[0]
    each = 32 // parts
    copies = [
        pltpu.make_async_copy(w_hbm.at[pl.ds(each * i, each)], w_ref.at[pl.ds(each * i, each)], sems.at[i])
        for i in range(parts)
    ]
    for copy in copies:
        copy.start()
    deep = 64 * each
    for i in range(parts):
        copies[i].wait()
        for c in range(2):
            w = w_ref[each * i : each * (i + 1), c, :, 0:1408].reshape(deep, 1408)
            d = jnp.dot(x_ref[:, deep * i : deep * (i + 1)], w, preferred_element_type=F32)
            if i == 0:
                gu[c] = d
            else:
                gu[c] += d
    for c in range(2):
        hid[:, 768 * c : 768 * c + 640] = (jax.nn.silu(gu[c, :, 0:640]) * gu[c, :, 640:1280]).astype(BF)
        tail = gu[c, :, 1280:1408]
        both = jax.nn.silu(tail) * pltpu.roll(tail, 64, 1)
        lane = lax.broadcasted_iota(jnp.int32, both.shape, 1)
        hid[:, 768 * c + 640 : 768 * c + 768] = jnp.where(lane < 64, both, 0.0).astype(BF)
    for n in range(8):
        total = None
        for c in range(2):
            w = w_ref[4 * n : 4 * (n + 1), c, :, 1408:2176].reshape(256, 768)
            d = lax.dot_general(
                hid[:, 768 * c : 768 * (c + 1)], w, (((1,), (1,)), ((), ())), preferred_element_type=F32
            )
            total = d if total is None else total + d
        out_ref[:, 256 * n : 256 * (n + 1)] = total.astype(BF)


def mixer(x, w):
    rows = x.shape[0]
    return pl.pallas_call(
        mixer_body,
        in_specs=[*whole(1), pl.BlockSpec(memory_space=pl.ANY)],
        out_specs=pl.BlockSpec(memory_space=pltpu.VMEM),
        out_shape=jax.ShapeDtypeStruct((rows, 2048), BF),
        scratch_shapes=[
            pltpu.VMEM(w.shape, BF),
            pltpu.VMEM((2, rows, 1408), F32),
            pltpu.VMEM((rows, 1536), BF),
            pltpu.SemaphoreType.DMA((4,)),
        ],
        compiler_params=pltpu.CompilerParams(vmem_limit_bytes=48 * 2**20),
        cost_estimate=pl.CostEstimate(flops=6 * rows * 2048 * 1408, bytes_accessed=18 * 2**20, transcendentals=0),
        name="mixer",
    )(x, w)


def swap(v):
    return lax.ppermute(v, "c", [(0, 1), (1, 0)])


def around(v, step):
    return lax.ppermute(v, "z", [(i, (i + step) % Z) for i in range(Z)])


def exchange(v, axis):
    return lax.all_to_all(v, axis, split_axis=0, concat_axis=0, tiled=True)


def body(residual, queries, keys, values, mix_lambda, head_gain, out_weight, norm_gain, gate, up, down):
    x, y, c = lax.axis_index("x"), lax.axis_index("y"), lax.axis_index("c")

    packed = small(pack_body, "pack", ((64, 2176), BF), 0, gate, up, down)
    weights = lax.all_gather(packed, ("z", "y", "c"), axis=0, tiled=False).reshape(32, 2, 64, 2176)

    core = c.reshape(1)
    got = swap(small(send_body, "send", ((768, 256), BF), 1, core, queries, keys, values))
    heads = small(heads_body, "heads", ((Y, 768, 128), BF), 1, core, queries, keys, values, got)
    head = exchange(heads, "y")
    block = small(block_body, "block", ((1536, 128), BF), 0, head)
    right, left = around(block, 1), around(block, -1)
    q_all = small(queries_body, "queries", ((3072, 128), BF), 1, core, head)

    one = [(0, 0, 384), (0, 768, 1152)]
    two = one + [(1, 0, 384), (1, 768, 1152)]
    states = attend(q_all, [block], one, None)
    right2, left2 = around(right, 1), around(left, -1)
    states = attend(q_all, [right, left], two, states)
    right3, left3 = around(right2, 1), around(left2, -1)
    states = attend(q_all, [right2, left2], two, states)
    last_r, last_l = around(right3[:768], 1), around(left3[768:], -1)
    states = attend(q_all, [right3, left3], two, states)
    ends = [(0, 0, 384), (1, 0, 384)]
    (theirs,) = attend(q_all, [last_r, last_l], ends, states[:1], 1)
    other = swap(theirs)
    (own,) = attend(q_all, [last_r, last_l], ends, states[1:], 1, 6)

    lam_got = swap(mix_lambda)
    lam4 = jnp.where(c == 0, jnp.concatenate([mix_lambda, lam_got]), jnp.concatenate([lam_got, mix_lambda]))
    lam = lax.dynamic_slice_in_dim(lam4, y, 1, 0)
    attended = finish(own, other, lam, head_gain.reshape(1, 128))

    heads = exchange(attended.reshape(Y, 192, 128), "y")
    w_got = swap(out_weight)
    a_mine = lax.dynamic_slice_in_dim(heads, 2 * c, 2, 0)
    a_other = lax.dynamic_slice_in_dim(heads, 2 - 2 * c, 2, 0)
    side = lambda a: jnp.concatenate([a[0], a[1]], axis=1)
    part = jnp.dot(side(a_mine), out_weight, preferred_element_type=F32) + jnp.dot(
        side(a_other), w_got, preferred_element_type=F32
    )
    projected = exchange(part.astype(BF).reshape(X, 48, 2048), "x").astype(F32).sum(axis=0)
    after_mix = residual.astype(F32) + projected
    scale = lax.rsqrt(jnp.mean(after_mix * after_mix, axis=-1, keepdims=True) + 1e-06)
    normed = (after_mix * scale * norm_gain).astype(BF)
    rows = exchange(jnp.broadcast_to(normed, (X, 48, 2048)), "x").reshape(192, 2048)
    mixed = exchange(mixer(rows, weights).reshape(X, 48, 2048), "x").astype(F32).sum(axis=0)
    return (after_mix + 0.5 * mixed).astype(BF)


def solution(mesh):
    split = Mesh(mesh.devices.reshape(Z, Y, X, C), ("z", "y", "x", "c"))
    sp, tp = ("z", "y"), ("x", "c")
    return jax.shard_map(
        body,
        mesh=split,
        in_specs=(
            P(("z", "y", "x", "c"), None),
            P(sp, tp),
            P(sp, tp),
            P(sp, tp),
            P(tp),
            P(),
            P(tp, None),
            P(),
            P(sp, tp),
            P(sp, tp),
            P(tp, sp),
        ),
        out_specs=P(("z", "y", "x", "c"), None),
        check_vma=False,
    )
```

```python
import functools

import jax
import jax.numpy as jnp
from jax import lax
from jax.experimental import pallas as pl
from jax.experimental.pallas import tpu as pltpu
from jax.sharding import Mesh, PartitionSpec as P


BF = jnp.bfloat16
F32 = jnp.float32
Z, Y, X, C = 8, 4, 4, 2
TQ = 256


def whole(n):
    return [pl.BlockSpec(memory_space=pltpu.VMEM)] * n


def attend_body(*refs, pieces, first, parts, start):
    count = 1 + max(p[0] for p in pieces)
    q_ref, kv_refs = refs[0], refs[1 : 1 + count]
    old_refs = [None] * parts if first else refs[1 + count : 1 + count + parts]
    new_refs = refs[-2 - parts : -2]
    sa, sb = refs[-2:]
    each = new_refs[0].shape[1] // TQ
    tiles = each * parts

    def scores(t, s):
        q = q_ref[pl.ds(pl.multiple_of((start + t) * TQ, TQ), TQ), :]
        top = None
        for j, (which, row, _) in enumerate(pieces):
            d = lax.dot_general(
                kv_refs[which][row : row + 384, :], q, (((1,), (1,)), ((), ())), preferred_element_type=F32
            )
            s[384 * j : 384 * (j + 1), :] = d
            m = jnp.max(d.reshape(48, 8, TQ), axis=0)
            top = m if top is None else jnp.maximum(top, m)
        return jnp.max(top, axis=0, keepdims=True)

    def add(t, s, top, old_ref, new_ref):
        at = pl.ds(pl.multiple_of(t * TQ, TQ), TQ)
        if not first:
            old_top = old_ref[136:137, at]
            top = jnp.maximum(old_top, top)
        total = None
        for j in range(0, len(pieces), 2):
            p = jnp.exp(s[384 * j : 384 * (j + 2), :] - top).astype(BF)
            v = jnp.concatenate(
                [kv_refs[w][row + 128 * i : row + 128 * (i + 1), :] for w, _, row in pieces[j : j + 2] for i in range(3)],
                axis=1,
            )
            ones = jnp.ones((16, 768), BF)
            d = jnp.dot(jnp.concatenate([v, ones], axis=0), p, preferred_element_type=F32)
            total = d if total is None else total + d
        total = total[:136]
        if not first:
            total = old_ref[0:136, at] * jnp.exp(old_top - top) + total
        new_ref[0:136, at] = total
        new_ref[136:144, at] = jnp.broadcast_to(top, (8, TQ))

    top = scores(0, sa)
    for part in range(parts):

        def body(i, top):
            t = 2 * i
            base = each * part
            top_b = scores(base + t + 1, sb)
            add(t, sa, top, old_refs[part], new_refs[part])
            top_a = scores(jnp.minimum(base + t + 2, tiles - 1), sa)
            add(t + 1, sb, top_b, old_refs[part], new_refs[part])
            return top_a

        top = lax.fori_loop(0, each // 2, body, top)


def attend(q, arrays, pieces, states, parts=2, start=0):
    first = states is None
    n = 1536 * parts
    keys = 384 * len(pieces)
    args = [q, *arrays] + ([] if first else list(states))
    return pl.pallas_call(
        functools.partial(attend_body, pieces=pieces, first=first, parts=parts, start=start),
        in_specs=whole(len(args)),
        out_specs=whole(parts),
        out_shape=[jax.ShapeDtypeStruct((144, n // parts), F32)] * parts,
        scratch_shapes=[pltpu.VMEM((keys, TQ), F32)] * 2,
        input_output_aliases={} if first else {len(args) - parts + i: i for i in range(parts)},
        compiler_params=pltpu.CompilerParams(vmem_limit_bytes=16 * 2**20),
        cost_estimate=pl.CostEstimate(flops=8 * 256 * n * keys, bytes_accessed=2**22, transcendentals=n * keys),
        name="attend",
    )(*args)


def pack_body(gate_hbm, up_hbm, down_hbm, out_ref, gate_ref, up_ref, down_ref, sems):
    copies = [
        pltpu.make_async_copy(a, b, sems.at[i])
        for i, (a, b) in enumerate(((gate_hbm, gate_ref), (up_hbm, up_ref), (down_hbm, down_ref)))
    ]
    for copy in copies:
        copy.start()
    for copy in copies:
        copy.wait()
    for i, (a, b) in enumerate(((0, 256), (256, 512), (512, 640))):
        out_ref[:, 512 * i : 512 * i + b - a] = gate_ref[:, a:b]
        out_ref[:, 512 * i + b - a : 512 * i + 2 * (b - a)] = up_ref[:, a:b]
    tails = [r[:, 640:704].astype(F32) for r in (gate_ref, up_ref)]
    out_ref[:, 1280:1408] = jnp.concatenate(tails, axis=1).astype(BF)
    out_ref[:, 1408:2048] = down_ref[:, 0:640]
    last = jnp.concatenate([down_ref[:, 640:704].astype(F32), jnp.zeros((64, 64), F32)], axis=1)
    out_ref[:, 2048:2176] = last.astype(BF)


def pack(gate, up, down):
    return pl.pallas_call(
        pack_body,
        in_specs=[pl.BlockSpec(memory_space=pltpu.HBM)] * 3,
        out_specs=pl.BlockSpec(memory_space=pltpu.VMEM),
        out_shape=jax.ShapeDtypeStruct((64, 2176), BF),
        scratch_shapes=[
            pltpu.VMEM((64, 704), BF),
            pltpu.VMEM((64, 704), BF),
            pltpu.VMEM((64, 704), BF),
            pltpu.SemaphoreType.DMA((3,)),
        ],
        compiler_params=pltpu.CompilerParams(vmem_limit_bytes=63 * 2**20),
        cost_estimate=pl.CostEstimate(flops=10**7, bytes_accessed=2**19, transcendentals=0),
        name="pack",
    )(gate, up, down)


def small(body, shapes, scalars, *args):
    alone = not isinstance(shapes, list)
    return pl.pallas_call(
        body,
        in_specs=[pl.BlockSpec(memory_space=pltpu.SMEM)] * scalars + whole(len(args) - scalars),
        out_specs=pl.BlockSpec(memory_space=pltpu.VMEM) if alone else whole(len(shapes)),
        out_shape=jax.ShapeDtypeStruct(*shapes) if alone else [jax.ShapeDtypeStruct(*sh) for sh in shapes],
        compiler_params=pltpu.CompilerParams(vmem_limit_bytes=8 * 2**20),
        cost_estimate=pl.CostEstimate(flops=10**7, bytes_accessed=2**20, transcendentals=0),
    )(*args)


def send_body(c_ref, q_ref, k_ref, v_ref, out_ref):
    put_half(1 - c_ref[0], q_ref, k_ref, v_ref, lambda rows, ref, at: out_ref.__setitem__((rows, slice(None)), ref[at, :]))


def put_half(sub, q_ref, k_ref, v_ref, put):
    for x in range(4):
        put(slice(48 * x, 48 * (x + 1)), q_ref, pl.ds(pl.multiple_of(96 * x + 48 * sub, 48), 48))
    for i, ref in ((1, k_ref), (2, v_ref)):
        put(slice(192 * i, 192 * (i + 1)), ref, pl.ds(pl.multiple_of(192 * sub, 192), 192))


def heads_body(c_ref, q_ref, k_ref, v_ref, got_ref, out_ref):
    c = c_ref[0]
    for j in range(2):
        lanes = slice(128 * j, 128 * (j + 1))

        def put(rows, ref, at):
            out_ref[2 * c + j, rows, :] = ref[at, lanes]

        put_half(c, q_ref, k_ref, v_ref, put)
        out_ref[2 - 2 * c + j] = got_ref[:, lanes]


def block_body(head_ref, block_ref, q_ref):
    for i in range(4):
        at = 768 * (i // 2) + 192 * (i % 2)
        block_ref[at : at + 192, :] = head_ref[i, 192:384, :]
        q_ref[192 * i : 192 * (i + 1), :] = head_ref[i, 0:192, :]
    values = jnp.concatenate([head_ref[i, 384:576, :] for i in range(4)], axis=0)
    for i in range(6):
        at = 768 * (i // 3) + 384 + 128 * (i % 3)
        block_ref[at : at + 128, :] = values[128 * i : 128 * (i + 1), :].T


def queries_body(other_ref, own_ref, out_ref):
    lane = lax.broadcasted_iota(jnp.int32, (768, 128), 1)
    for i, ref in enumerate((other_ref, own_ref)):
        rows = ref[...].astype(F32) * 0.125
        out_ref[1536 * i : 1536 * i + 768, :] = jnp.where(lane < 64, rows, 0.0).astype(BF)
        out_ref[1536 * i + 768 : 1536 * (i + 1), :] = jnp.where(lane < 64, 0.0, rows).astype(BF)


def carry_body(w_ref, r_ref, out_ref):
    out_ref[0:128, :] = w_ref[0:128, :]
    out_ref[128:160, :] = r_ref[0:32, :]
    out_ref[160:288, :] = w_ref[128:256, :]
    out_ref[288:304, :] = r_ref[32:48, :]


def finish_body(mine_ref, other_ref, lam_ref, gain_ref, out_ref):
    n = 768
    lam = lam_ref[0]
    gain = gain_ref[...]
    for t in range(n // 128):
        maps = []
        for comp in range(2):
            at = slice(n * comp + 128 * t, n * comp + 128 * (t + 1))
            m0, m1 = mine_ref[136:137, at], other_ref[136:137, at]
            top = jnp.maximum(m0, m1)
            w0, w1 = jnp.exp(m0 - top), jnp.exp(m1 - top)
            total = mine_ref[128:129, at] * w0 + other_ref[128:129, at] * w1
            maps.append((mine_ref[0:128, at] * w0 + other_ref[0:128, at] * w1) / total)
        mixed = maps[0] - lam * maps[1]
        scale = lax.rsqrt(jnp.mean(mixed * mixed, axis=0, keepdims=True) + 1e-06)
        rows = ((mixed * scale).T * gain).astype(BF)
        for at in (128 * t, 128 * t + 64):
            for x in range(4):
                out_ref[at // 192, x, at % 192 : at % 192 + 64, :] = rows[at - 128 * t : at - 128 * t + 64]


def finish(mine, other, lam, gain):
    return pl.pallas_call(
        finish_body,
        in_specs=[*whole(2), pl.BlockSpec(memory_space=pltpu.SMEM), *whole(1)],
        out_specs=pl.BlockSpec(memory_space=pltpu.VMEM),
        out_shape=jax.ShapeDtypeStruct((Y, X, 192, 128), BF),
        compiler_params=pltpu.CompilerParams(vmem_limit_bytes=8 * 2**20),
        cost_estimate=pl.CostEstimate(flops=10**8, bytes_accessed=2**21, transcendentals=0),
        name="finish",
    )(mine, other, lam, gain)


def project_body(at_ref, g_ref, gain_ref, *refs):
    hbm, (normed_ref, own_ref, po, acc, sems) = refs[:10], refs[10:]
    x, c = at_ref[0], at_ref[1]
    copies = []
    for half in range(2):
        lanes = slice(1024 * half, 1024 * (half + 1))
        for i, ref in enumerate(hbm):
            k, rows = (i, slice(0, 304)) if i < 6 else (6 + i % 2, slice(0, 160) if i < 8 else slice(160, 304))
            copies.append(pltpu.make_async_copy(ref.at[:, lanes], po.at[k, rows, lanes], sems.at[10 * half + i]))
    for copy in copies:
        copy.start()
    blocks = []
    for k in range(8):
        xk = lax.rem(x + 4 + (0, -1, 1, 2)[k // 2], 4)
        ck = c if k % 2 == 0 else 1 - c
        blocks.append(jnp.concatenate([g_ref[2 * ck, xk], g_ref[2 * ck + 1, xk]], axis=1))
    for half in range(2):
        for i in range(10):
            copies[10 * half + i].wait()
        for n in range(2):
            lanes = slice(1024 * half + 512 * n, 1024 * half + 512 * (n + 1))
            total = None
            for k, a in enumerate(blocks):
                w = jnp.concatenate([po[k, 0:128, lanes], po[k, 160:288, lanes]], axis=0)
                d = jnp.dot(a, w, preferred_element_type=F32)
                total = d if total is None else total + d
            acc[:, lanes] = total
    for k, step in ((0, 0), (2, -1), (4, 1), (6, 2)):
        at = 48 * lax.rem(x + 4 + step, 4)
        acc[pl.ds(pl.multiple_of(at, 16), 32), :] += po[k, 128:160, :].astype(F32)
        acc[pl.ds(pl.multiple_of(at + 32, 16), 16), :] += po[k, 288:304, :].astype(F32)
    own_ref[...] = acc[pl.ds(pl.multiple_of(48 * x, 16), 48), :]
    gain = gain_ref[...]
    for i in range(6):
        rows = acc[32 * i : 32 * (i + 1), :]
        scale = lax.rsqrt(jnp.mean(rows * rows, axis=1, keepdims=True) + 1e-06)
        normed_ref[32 * i : 32 * (i + 1), :] = (rows * scale * gain).astype(BF)


def project(at, g, gain, blocks):
    return pl.pallas_call(
        project_body,
        in_specs=[pl.BlockSpec(memory_space=pltpu.SMEM), *whole(2)] + [pl.BlockSpec(memory_space=pltpu.HBM)] * 10,
        out_specs=whole(2),
        out_shape=[jax.ShapeDtypeStruct((192, 2048), BF), jax.ShapeDtypeStruct((48, 2048), F32)],
        scratch_shapes=[
            pltpu.VMEM((8, 304, 2048), BF),
            pltpu.VMEM((192, 2048), F32),
            pltpu.SemaphoreType.DMA((20,)),
        ],
        compiler_params=pltpu.CompilerParams(vmem_limit_bytes=62 * 2**20),
        cost_estimate=pl.CostEstimate(flops=2 * 192 * 2048 * 2048, bytes_accessed=10 * 2**20, transcendentals=0),
        name="project",
    )(at, g, gain, *blocks)


def mixer_body(x_ref, w_hbm, out_ref, w_ref, hid, sems):
    chunks = [(c, a, b) for c in range(2) for a, b in ((0, 512), (512, 1024), (1024, 1408))]
    views = [(slice(None), c, slice(None), slice(a, b)) for c, a, b in chunks]
    views += [(slice(16 * i, 16 * (i + 1)), slice(None), slice(None), slice(1408, 2176)) for i in range(2)]
    copies = [pltpu.make_async_copy(w_hbm.at[v], w_ref.at[v], sems.at[i]) for i, v in enumerate(views)]
    for copy in copies:
        copy.start()
    for i, (c, a, b) in enumerate(chunks):
        copies[i].wait()
        gu = jnp.dot(x_ref[...], w_ref[:, c, :, a:b].reshape(2048, b - a), preferred_element_type=F32)
        n = 256 if b - a == 512 else 128
        at = 768 * c + a // 2
        hid[:, at : at + n] = (jax.nn.silu(gu[:, 0:n]) * gu[:, n : 2 * n]).astype(BF)
        if n == 128:
            tail = gu[:, 256:384]
            both = jax.nn.silu(tail) * pltpu.roll(tail, 64, 1)
            lane = lax.broadcasted_iota(jnp.int32, both.shape, 1)
            hid[:, at + 128 : at + 256] = jnp.where(lane < 64, both, 0.0).astype(BF)
    for half in range(2):
        copies[6 + half].wait()

        @pl.loop(2 * half, 2 * half + 2)
        def _(m):
            for part in range(2):
                total = None
                for c in range(2):
                    w = w_ref[pl.ds(8 * m + 4 * part, 4), c, :, 1408:2176].reshape(256, 768)
                    d = lax.dot_general(
                        hid[:, 768 * c : 768 * (c + 1)], w, (((1,), (1,)), ((), ())), preferred_element_type=F32
                    )
                    total = d if total is None else total + d
                out_ref[:, pl.ds(pl.multiple_of(512 * m + 256 * part, 256), 256)] = total.astype(BF)


def mixer(x, w):
    rows = x.shape[0]
    return pl.pallas_call(
        mixer_body,
        in_specs=[*whole(1), pl.BlockSpec(memory_space=pltpu.HBM)],
        out_specs=pl.BlockSpec(memory_space=pltpu.VMEM),
        out_shape=jax.ShapeDtypeStruct((rows, 2048), BF),
        scratch_shapes=[pltpu.VMEM(w.shape, BF), pltpu.VMEM((rows, 1536), BF), pltpu.SemaphoreType.DMA((8,))],
        compiler_params=pltpu.CompilerParams(vmem_limit_bytes=62 * 2**20),
        cost_estimate=pl.CostEstimate(flops=6 * rows * 2048 * 1408, bytes_accessed=18 * 2**20, transcendentals=0),
        name="mixer",
    )(x, w)


def swap(v):
    return lax.ppermute(v, "c", [(0, 1), (1, 0)])


def around(v, step, axis="z", n=Z):
    return lax.ppermute(v, axis, [(i, (i + step) % n) for i in range(n)])


def exchange(v, axis):
    return lax.all_to_all(v, axis, split_axis=0, concat_axis=0, tiled=True)


def inner(residual, queries, keys, values, mix_lambda, head_gain, out_weight, norm_gain, gate, up, down):
    x, y, c = lax.axis_index("x"), lax.axis_index("y"), lax.axis_index("c")

    packed = pack(gate, up, down.T)
    weights = lax.all_gather(packed, ("z", "y", "c"), axis=0, tiled=False).reshape(32, 2, 64, 2176)

    core = c.reshape(1)
    lam_got = swap(mix_lambda)
    got = swap(small(send_body, ((576, 256), BF), 1, core, queries, keys, values))
    heads = small(heads_body, ((Y, 576, 128), BF), 1, core, queries, keys, values, got)
    head = exchange(heads, "y")
    block, q_own = small(block_body, [((1536, 128), BF), ((768, 128), BF)], 0, head)
    right, left = around(block, 1), around(block, -1)
    q_all = small(queries_body, ((3072, 128), BF), 0, swap(q_own), q_own)
    lam4 = jnp.where(c == 0, jnp.concatenate([mix_lambda, lam_got]), jnp.concatenate([lam_got, mix_lambda]))
    lam = lax.dynamic_slice_in_dim(lam4, y, 1, 0)

    at = jnp.stack([x, c])
    q_all, lam, at, out_weight, residual = lax.optimization_barrier((q_all, lam, at, out_weight, residual))
    carry = small(carry_body, ((304, 2048), BF), 0, out_weight, residual)
    from_left, from_right = around(carry, 1, "x", X), around(carry, -1, "x", X)
    carry_c = swap(carry)

    one = [(0, 0, 384), (0, 768, 1152)]
    two = one + [(1, 0, 384), (1, 768, 1152)]
    after = lax.optimization_barrier
    states = attend(q_all, [block], one, None)
    states, right, left = after((states, right, left))
    right2, left2 = around(right, 1), around(left, -1)
    states = attend(q_all, [right, left], two, states)
    states, right2, left2 = after((states, right2, left2))
    right3, left3 = around(right2, 1), around(left2, -1)
    states, from_left, from_right, carry_c = after((states, from_left, from_right, carry_c))
    far_a, far_b = around(from_left[:160], 1, "x", X), around(from_right[160:], -1, "x", X)
    left_c, right_c = swap(from_left), swap(from_right)
    states = attend(q_all, [right2, left2], two, states)
    states, right3, left3 = after((states, right3, left3))
    last_r, last_l = around(right3[:768], 1), around(left3[768:], -1)
    states, far_a, far_b, left_c, right_c = after((states, far_a, far_b, left_c, right_c))
    far_a_c, far_b_c = swap(far_a), swap(far_b)
    states = attend(q_all, [right3, left3], two, states)
    states, last_r, last_l, far_a_c, far_b_c = after((states, last_r, last_l, far_a_c, far_b_c))
    ends = [(0, 0, 384), (1, 0, 384)]
    (theirs,) = attend(q_all, [last_r, last_l], ends, states[:1], 1)
    other = swap(theirs)
    (own,) = attend(q_all, [last_r, last_l], ends, states[1:], 1, 6)

    attended = finish(own, other, lam, head_gain.reshape(1, 128)).reshape(Y * X, 192, 128)
    spread = exchange(attended, ("y", "x")).reshape(Y, X, 192, 128)
    blocks = [carry, carry_c, from_left, left_c, from_right, right_c, far_a, far_a_c, far_b, far_b_c]
    spread, weights = after((spread, weights))
    rows, after_mix = project(at, spread, norm_gain.reshape(1, 2048), blocks)
    mixed = mixer(rows, weights)
    mixed = exchange(mixed.reshape(X, 48, 2048), "x").astype(F32).sum(axis=0)
    return (after_mix + 0.5 * mixed).astype(BF)


def solution(mesh):
    split = Mesh(mesh.devices.reshape(Z, Y, X, C), ("z", "y", "x", "c"))
    sp, tp = ("z", "y"), ("x", "c")
    return jax.shard_map(
        inner,
        mesh=split,
        in_specs=(
            P(("z", "y", "x", "c"), None),
            P(sp, tp),
            P(sp, tp),
            P(sp, tp),
            P(tp),
            P(),
            P(tp, None),
            P(),
            P(sp, tp),
            P(sp, tp),
            P(tp, sp),
        ),
        out_specs=P(("z", "y", "x", "c"), None),
        check_vma=False,
    )
```

```python
import functools

import jax
import jax.numpy as jnp
from jax import lax
from jax.experimental import pallas as pl
from jax.experimental.pallas import tpu as pltpu
from jax.sharding import Mesh, PartitionSpec as P


BF = jnp.bfloat16
F32 = jnp.float32
Z, Y, X, C = 8, 4, 4, 2
TQ = 256


def whole(n):
    return [pl.BlockSpec(memory_space=pltpu.VMEM)] * n


def attend_body(*refs, pieces, first, parts, start):
    count = 1 + max(p[0] for p in pieces)
    q_ref, kv_refs = refs[0], refs[1 : 1 + count]
    old_refs = [None] * parts if first else refs[1 + count : 1 + count + parts]
    new_refs = refs[-2 - parts : -2]
    sa, sb = refs[-2:]
    each = new_refs[0].shape[1] // TQ
    tiles = each * parts

    def scores(t, s):
        q = q_ref[pl.ds(pl.multiple_of((start + t) * TQ, TQ), TQ), :]
        top = None
        for j, (which, row, _) in enumerate(pieces):
            d = lax.dot_general(
                kv_refs[which][row : row + 384, :], q, (((1,), (1,)), ((), ())), preferred_element_type=F32
            )
            s[384 * j : 384 * (j + 1), :] = d
            m = jnp.max(d.reshape(48, 8, TQ), axis=0)
            top = m if top is None else jnp.maximum(top, m)
        return jnp.max(top, axis=0, keepdims=True)

    def add(t, s, top, old_ref, new_ref):
        at = pl.ds(pl.multiple_of(t * TQ, TQ), TQ)
        if not first:
            old_top = old_ref[136:137, at]
            top = jnp.maximum(old_top, top)
        total = None
        for j in range(0, len(pieces), 2):
            p = jnp.exp(s[384 * j : 384 * (j + 2), :] - top).astype(BF)
            v = jnp.concatenate(
                [kv_refs[w][row + 128 * i : row + 128 * (i + 1), :] for w, _, row in pieces[j : j + 2] for i in range(3)],
                axis=1,
            )
            ones = jnp.ones((16, 768), BF)
            d = jnp.dot(jnp.concatenate([v, ones], axis=0), p, preferred_element_type=F32)
            total = d if total is None else total + d
        total = total[:136]
        if not first:
            total = old_ref[0:136, at] * jnp.exp(old_top - top) + total
        new_ref[0:136, at] = total
        new_ref[136:144, at] = jnp.broadcast_to(top, (8, TQ))

    top = scores(0, sa)
    for part in range(parts):

        def body(i, top):
            t = 2 * i
            base = each * part
            top_b = scores(base + t + 1, sb)
            add(t, sa, top, old_refs[part], new_refs[part])
            top_a = scores(jnp.minimum(base + t + 2, tiles - 1), sa)
            add(t + 1, sb, top_b, old_refs[part], new_refs[part])
            return top_a

        top = lax.fori_loop(0, each // 2, body, top)


def attend(q, arrays, pieces, states, parts=2, start=0):
    first = states is None
    n = 1536 * parts
    keys = 384 * len(pieces)
    args = [q, *arrays] + ([] if first else list(states))
    return pl.pallas_call(
        functools.partial(attend_body, pieces=pieces, first=first, parts=parts, start=start),
        in_specs=whole(len(args)),
        out_specs=whole(parts),
        out_shape=[jax.ShapeDtypeStruct((144, n // parts), F32)] * parts,
        scratch_shapes=[pltpu.VMEM((keys, TQ), F32)] * 2,
        input_output_aliases={} if first or parts == 1 else {len(args) - parts + i: i for i in range(parts)},
        compiler_params=pltpu.CompilerParams(vmem_limit_bytes=16 * 2**20),
        cost_estimate=pl.CostEstimate(flops=8 * 256 * n * keys, bytes_accessed=2**22, transcendentals=n * keys),
        name="attend",
    )(*args)


def pack_body(gate_hbm, up_hbm, down_hbm, out_ref, gate_ref, up_ref, down_ref, sems):
    copies = [
        pltpu.make_async_copy(a, b, sems.at[i])
        for i, (a, b) in enumerate(((gate_hbm, gate_ref), (up_hbm, up_ref), (down_hbm, down_ref)))
    ]
    for copy in copies:
        copy.start()
    for copy in copies:
        copy.wait()
    for i, (a, b) in enumerate(((0, 256), (256, 512), (512, 640))):
        out_ref[:, 512 * i : 512 * i + b - a] = gate_ref[:, a:b]
        out_ref[:, 512 * i + b - a : 512 * i + 2 * (b - a)] = up_ref[:, a:b]
    tails = [r[:, 640:704].astype(F32) for r in (gate_ref, up_ref)]
    out_ref[:, 1280:1408] = jnp.concatenate(tails, axis=1).astype(BF)
    out_ref[:, 1408:2048] = down_ref[:, 0:640]
    last = jnp.concatenate([down_ref[:, 640:704].astype(F32), jnp.zeros((64, 64), F32)], axis=1)
    out_ref[:, 2048:2176] = last.astype(BF)


def pack(gate, up, down):
    return pl.pallas_call(
        pack_body,
        in_specs=[pl.BlockSpec(memory_space=pltpu.HBM)] * 3,
        out_specs=pl.BlockSpec(memory_space=pltpu.VMEM),
        out_shape=jax.ShapeDtypeStruct((64, 2176), BF),
        scratch_shapes=[
            pltpu.VMEM((64, 704), BF),
            pltpu.VMEM((64, 704), BF),
            pltpu.VMEM((64, 704), BF),
            pltpu.SemaphoreType.DMA((3,)),
        ],
        compiler_params=pltpu.CompilerParams(vmem_limit_bytes=63 * 2**20),
        cost_estimate=pl.CostEstimate(flops=10**7, bytes_accessed=2**19, transcendentals=0),
        name="pack",
    )(gate, up, down)


def small(body, shapes, scalars, *args):
    alone = not isinstance(shapes, list)
    return pl.pallas_call(
        body,
        in_specs=[pl.BlockSpec(memory_space=pltpu.SMEM)] * scalars + whole(len(args) - scalars),
        out_specs=pl.BlockSpec(memory_space=pltpu.VMEM) if alone else whole(len(shapes)),
        out_shape=jax.ShapeDtypeStruct(*shapes) if alone else [jax.ShapeDtypeStruct(*sh) for sh in shapes],
        compiler_params=pltpu.CompilerParams(vmem_limit_bytes=8 * 2**20),
        cost_estimate=pl.CostEstimate(flops=10**7, bytes_accessed=2**20, transcendentals=0),
    )(*args)


def send_body(c_ref, q_hbm, k_hbm, v_hbm, own_ref, out_ref, q_ref, k_ref, v_ref, sems):
    pairs = ((q_hbm, q_ref), (k_hbm, k_ref), (v_hbm, v_ref))
    copies = [pltpu.make_async_copy(a, b, sems.at[i]) for i, (a, b) in enumerate(pairs)]
    for copy in copies:
        copy.start()
    for copy in copies:
        copy.wait()
    c = c_ref[0]
    for sub, to_ref in ((c, own_ref), (1 - c, out_ref)):
        for x in range(4):
            to_ref[48 * x : 48 * (x + 1), :] = q_ref[pl.ds(pl.multiple_of(96 * x + 48 * sub, 48), 48), :]
        at = pl.ds(pl.multiple_of(192 * sub, 192), 192)
        to_ref[192:384, :] = k_ref[at, :]
        to_ref[384:576, :] = v_ref[at, :]


def send(core, q, k, v):
    half = jax.ShapeDtypeStruct((576, 256), BF)
    return pl.pallas_call(
        send_body,
        in_specs=[pl.BlockSpec(memory_space=pltpu.SMEM)] + [pl.BlockSpec(memory_space=pltpu.HBM)] * 3,
        out_specs=whole(2),
        out_shape=[half, half],
        scratch_shapes=[pltpu.VMEM((384, 256), BF)] * 3 + [pltpu.SemaphoreType.DMA((3,))],
        compiler_params=pltpu.CompilerParams(vmem_limit_bytes=63 * 2**20),
        cost_estimate=pl.CostEstimate(flops=10**7, bytes_accessed=2**20, transcendentals=0),
        name="send",
    )(core, q, k, v)


def heads_body(c_ref, own_ref, got_ref, out_ref):
    c = c_ref[0]
    for j in range(2):
        lanes = slice(128 * j, 128 * (j + 1))
        out_ref[2 * c + j] = own_ref[:, lanes]
        out_ref[2 - 2 * c + j] = got_ref[:, lanes]


def block_body(head_ref, block_ref, q_ref):
    for i in range(4):
        at = 768 * (i // 2) + 192 * (i % 2)
        block_ref[at : at + 192, :] = head_ref[i, 192:384, :]
        q_ref[192 * i : 192 * (i + 1), :] = head_ref[i, 0:192, :]
    values = jnp.concatenate([head_ref[i, 384:576, :] for i in range(4)], axis=0)
    for i in range(6):
        at = 768 * (i // 3) + 384 + 128 * (i % 3)
        block_ref[at : at + 128, :] = values[128 * i : 128 * (i + 1), :].T


def queries_body(other_ref, own_ref, out_ref):
    lane = lax.broadcasted_iota(jnp.int32, (768, 128), 1)
    for i, ref in enumerate((other_ref, own_ref)):
        rows = ref[...].astype(F32) * 0.125
        out_ref[1536 * i : 1536 * i + 768, :] = jnp.where(lane < 64, rows, 0.0).astype(BF)
        out_ref[1536 * i + 768 : 1536 * (i + 1), :] = jnp.where(lane < 64, 0.0, rows).astype(BF)


def carry_body(w_ref, r_ref, out_ref):
    out_ref[0:128, :] = w_ref[0:128, :]
    out_ref[128:160, :] = r_ref[0:32, :]
    out_ref[160:288, :] = w_ref[128:256, :]
    out_ref[288:304, :] = r_ref[32:48, :]


def finish_body(y_ref, c_ref, lam_ref, lam_got_ref, mine_ref, other_ref, gain_ref, out_ref):
    n = 768
    y, c = y_ref[0], c_ref[0]
    lam = jnp.where(c == y // 2, lam_ref[y % 2], lam_got_ref[y % 2])
    gain = gain_ref[...]
    for t in range(n // 128):
        maps = []
        for comp in range(2):
            at = slice(n * comp + 128 * t, n * comp + 128 * (t + 1))
            m0, m1 = mine_ref[136:137, at], other_ref[136:137, at]
            top = jnp.maximum(m0, m1)
            w0, w1 = jnp.exp(m0 - top), jnp.exp(m1 - top)
            total = mine_ref[128:129, at] * w0 + other_ref[128:129, at] * w1
            maps.append((mine_ref[0:128, at] * w0 + other_ref[0:128, at] * w1) / total)
        mixed = maps[0] - lam * maps[1]
        scale = lax.rsqrt(jnp.mean(mixed * mixed, axis=0, keepdims=True) + 1e-06)
        rows = ((mixed * scale).T * gain).astype(BF)
        for at in (128 * t, 128 * t + 64):
            for x in range(4):
                out_ref[at // 192, x, at % 192 : at % 192 + 64, :] = rows[at - 128 * t : at - 128 * t + 64]


def finish(y, c, lam, lam_got, mine, other, gain):
    return pl.pallas_call(
        finish_body,
        in_specs=[pl.BlockSpec(memory_space=pltpu.SMEM)] * 4 + whole(3),
        out_specs=pl.BlockSpec(memory_space=pltpu.VMEM),
        out_shape=jax.ShapeDtypeStruct((Y, X, 192, 128), BF),
        compiler_params=pltpu.CompilerParams(vmem_limit_bytes=8 * 2**20),
        cost_estimate=pl.CostEstimate(flops=10**8, bytes_accessed=2**21, transcendentals=0),
        name="finish",
    )(y, c, lam, lam_got, mine, other, gain)


def layer_body(x_ref, c_ref, g_ref, gain_ref, *refs):
    hbm, w_hbm = refs[:10], refs[10]
    out_ref, own_ref, po, wf, acc, xn, hid, sems = refs[11:]
    x, c = x_ref[0], c_ref[0]
    copies = []
    for half in range(2):
        lanes = slice(1024 * half, 1024 * (half + 1))
        for i, ref in enumerate(hbm):
            k, rows = (i, slice(0, 304)) if i < 6 else (6 + i % 2, slice(0, 160) if i < 8 else slice(160, 304))
            copies.append(pltpu.make_async_copy(ref.at[:, lanes], po.at[k, rows, lanes], sems.at[10 * half + i]))
    chunks = [(c2, a, b) for c2 in range(2) for a, b in ((0, 512), (512, 1024), (1024, 1408))]
    views = [(slice(None), c2, slice(None), slice(a, b)) for c2, a, b in chunks]
    views += [(slice(16 * i, 16 * (i + 1)), slice(None), slice(None), slice(1408, 2176)) for i in range(2)]
    streams = [pltpu.make_async_copy(w_hbm.at[v], wf.at[v], sems.at[20 + i]) for i, v in enumerate(views)]
    for copy in copies + streams:
        copy.start()

    blocks = []
    for k in range(8):
        xk = lax.rem(x + 4 + (0, -1, 1, 2)[k // 2], 4)
        ck = c if k % 2 == 0 else 1 - c
        blocks.append(jnp.concatenate([g_ref[2 * ck, xk], g_ref[2 * ck + 1, xk]], axis=1))
    for half in range(2):
        for copy in copies[10 * half : 10 * half + 10]:
            copy.wait()
        for n in range(2):
            lanes = slice(1024 * half + 512 * n, 1024 * half + 512 * (n + 1))
            total = None
            for k, a in enumerate(blocks):
                w = jnp.concatenate([po[k, 0:128, lanes], po[k, 160:288, lanes]], axis=0)
                d = jnp.dot(a, w, preferred_element_type=F32)
                total = d if total is None else total + d
            acc[:, lanes] = total
    for k, step in ((0, 0), (2, -1), (4, 1), (6, 2)):
        at = 48 * lax.rem(x + 4 + step, 4)
        acc[pl.ds(pl.multiple_of(at, 16), 32), :] += po[k, 128:160, :].astype(F32)
        acc[pl.ds(pl.multiple_of(at + 32, 16), 16), :] += po[k, 288:304, :].astype(F32)
    own_ref[...] = acc[pl.ds(pl.multiple_of(48 * x, 16), 48), :]
    gain = gain_ref[...]
    for i in range(6):
        rows = acc[32 * i : 32 * (i + 1), :]
        scale = lax.rsqrt(jnp.mean(rows * rows, axis=1, keepdims=True) + 1e-06)
        xn[32 * i : 32 * (i + 1), :] = (rows * scale * gain).astype(BF)

    for i, (c2, a, b) in enumerate(chunks):
        streams[i].wait()
        gu = jnp.dot(xn[...], wf[:, c2, :, a:b].reshape(2048, b - a), preferred_element_type=F32)
        n = 256 if b - a == 512 else 128
        at = 768 * c2 + a // 2
        hid[:, at : at + n] = (jax.nn.silu(gu[:, 0:n]) * gu[:, n : 2 * n]).astype(BF)
        if n == 128:
            tail = gu[:, 256:384]
            both = jax.nn.silu(tail) * pltpu.roll(tail, 64, 1)
            lane = lax.broadcasted_iota(jnp.int32, both.shape, 1)
            hid[:, at + 128 : at + 256] = jnp.where(lane < 64, both, 0.0).astype(BF)
    for half in range(2):
        streams[6 + half].wait()

        @pl.loop(2 * half, 2 * half + 2)
        def _(m):
            for part in range(2):
                total = None
                for c2 in range(2):
                    w = wf[pl.ds(8 * m + 4 * part, 4), c2, :, 1408:2176].reshape(256, 768)
                    d = lax.dot_general(
                        hid[:, 768 * c2 : 768 * (c2 + 1)], w, (((1,), (1,)), ((), ())), preferred_element_type=F32
                    )
                    total = d if total is None else total + d
                out_ref[:, pl.ds(pl.multiple_of(512 * m + 256 * part, 256), 256)] = total.astype(BF)


def layer(x, c, g, gain, blocks, w):
    return pl.pallas_call(
        layer_body,
        in_specs=[pl.BlockSpec(memory_space=pltpu.SMEM)] * 2
        + whole(2)
        + [pl.BlockSpec(memory_space=pltpu.HBM)] * 11,
        out_specs=whole(2),
        out_shape=[jax.ShapeDtypeStruct((192, 2048), BF), jax.ShapeDtypeStruct((48, 2048), F32)],
        scratch_shapes=[
            pltpu.VMEM((8, 304, 2048), BF),
            pltpu.VMEM(w.shape, BF),
            pltpu.VMEM((192, 2048), F32),
            pltpu.VMEM((192, 2048), BF),
            pltpu.VMEM((192, 1536), BF),
            pltpu.SemaphoreType.DMA((28,)),
        ],
        compiler_params=pltpu.CompilerParams(vmem_limit_bytes=62 * 2**20),
        cost_estimate=pl.CostEstimate(flops=8 * 192 * 2048 * 2048, bytes_accessed=28 * 2**20, transcendentals=0),
        name="layer",
    )(x, c, g, gain, *blocks, w)


def swap(v):
    return lax.ppermute(v, "c", [(0, 1), (1, 0)])


def around(v, step, axis="z", n=Z):
    return lax.ppermute(v, axis, [(i, (i + step) % n) for i in range(n)])


def exchange(v, axis):
    return lax.all_to_all(v, axis, split_axis=0, concat_axis=0, tiled=True)


def inner(residual, queries, keys, values, mix_lambda, head_gain, out_weight, norm_gain, gate, up, down):
    x, y, c = lax.axis_index("x"), lax.axis_index("y"), lax.axis_index("c")

    packed = pack(gate, up, down.T)
    weights = lax.all_gather(packed, ("z", "y", "c"), axis=0, tiled=False).reshape(32, 2, 64, 2176)

    core, x, y = c.reshape(1), x.reshape(1), y.reshape(1)
    after = lax.optimization_barrier
    kept, sent = send(core, queries, keys, values)
    heads = small(heads_body, ((Y, 576, 128), BF), 1, core, kept, swap(sent))
    head = exchange(heads, "y")

    heads, out_weight, residual = after((heads, out_weight, residual))
    carry = small(carry_body, ((304, 2048), BF), 0, out_weight, residual)
    from_left, from_right = around(carry, 1, "x", X), around(carry, -1, "x", X)
    carry_c = swap(carry)

    block, q_own = small(block_body, [((1536, 128), BF), ((768, 128), BF)], 0, head)
    right, left = around(block, 1), around(block, -1)
    q_other = swap(q_own)
    lam_got = swap(mix_lambda)
    q_all = small(queries_body, ((3072, 128), BF), 0, q_other, q_own)
    q_all, lam_got = after((q_all, lam_got))

    one = [(0, 0, 384), (0, 768, 1152)]
    two = one + [(1, 0, 384), (1, 768, 1152)]
    states = attend(q_all, [block], one, None)
    states, right, left = after((states, right, left))
    right2, left2 = around(right, 1), around(left, -1)
    states = attend(q_all, [right, left], two, states)
    states, right2, left2 = after((states, right2, left2))
    right3, left3 = around(right2, 1), around(left2, -1)
    states, from_left, from_right, carry_c = after((states, from_left, from_right, carry_c))
    far_a, far_b = around(from_left[:160], 1, "x", X), around(from_right[160:], -1, "x", X)
    left_c, right_c = swap(from_left), swap(from_right)
    states = attend(q_all, [right2, left2], two, states)
    states, right3, left3 = after((states, right3, left3))
    last_r, last_l = around(right3[:768], 1), around(left3[768:], -1)
    states, far_a, far_b, left_c, right_c = after((states, far_a, far_b, left_c, right_c))
    far_a_c, far_b_c = swap(far_a), swap(far_b)
    states = attend(q_all, [right3, left3], two, states)
    states, last_r, last_l, far_a_c, far_b_c = after((states, last_r, last_l, far_a_c, far_b_c))
    ends = [(0, 0, 384), (1, 0, 384)]
    (theirs,) = attend(q_all, [last_r, last_l], ends, states[:1], 1)
    other = swap(theirs)
    (own,) = attend(q_all, [last_r, last_l], ends, states[1:], 1, 6)

    attended = finish(y, core, mix_lambda, lam_got, own, other, head_gain.reshape(1, 128)).reshape(Y * X, 192, 128)
    spread = exchange(attended, ("y", "x")).reshape(Y, X, 192, 128)
    blocks = [carry, carry_c, from_left, left_c, from_right, right_c, far_a, far_a_c, far_b, far_b_c]
    spread, weights = after((spread, weights))
    mixed, after_mix = layer(x, core, spread, norm_gain.reshape(1, 2048), blocks, weights)
    mixed = exchange(mixed.reshape(X, 48, 2048), "x").astype(F32).sum(axis=0)
    return (after_mix + 0.5 * mixed).astype(BF)


def solution(mesh):
    split = Mesh(mesh.devices.reshape(Z, Y, X, C), ("z", "y", "x", "c"))
    sp, tp = ("z", "y"), ("x", "c")
    return jax.shard_map(
        inner,
        mesh=split,
        in_specs=(
            P(("z", "y", "x", "c"), None),
            P(sp, tp),
            P(sp, tp),
            P(sp, tp),
            P(tp),
            P(),
            P(tp, None),
            P(),
            P(sp, tp),
            P(sp, tp),
            P(tp, sp),
        ),
        out_specs=P(("z", "y", "x", "c"), None),
        check_vma=False,
    )
```

```python
import functools

import jax
import jax.numpy as jnp
from jax import lax
from jax.experimental import pallas as pl
from jax.experimental.pallas import tpu as pltpu
from jax.sharding import Mesh, PartitionSpec as P


BF = jnp.bfloat16
F32 = jnp.float32
Z, Y, X, C = 8, 4, 4, 2
TQ = 256


def whole(n):
    return [pl.BlockSpec(memory_space=pltpu.VMEM)] * n


def attend_body(*refs, pieces, first, parts, start):
    count = 1 + max(p[0] for p in pieces)
    q_ref, kv_refs = refs[0], refs[1 : 1 + count]
    old_refs = [None] * parts if first else refs[1 + count : 1 + count + parts]
    new_refs = refs[-2 - parts : -2]
    sa, sb = refs[-2:]
    each = new_refs[0].shape[1] // TQ
    tiles = each * parts

    def scores(t, s):
        q = q_ref[pl.ds(pl.multiple_of((start + t) * TQ, TQ), TQ), :]
        top = None
        for j, (which, row, _) in enumerate(pieces):
            d = lax.dot_general(
                kv_refs[which][row : row + 384, :], q, (((1,), (1,)), ((), ())), preferred_element_type=F32
            )
            s[384 * j : 384 * (j + 1), :] = d
            m = jnp.max(d.reshape(48, 8, TQ), axis=0)
            top = m if top is None else jnp.maximum(top, m)
        return jnp.max(top, axis=0, keepdims=True)

    def add(t, s, top, old_ref, new_ref):
        at = pl.ds(pl.multiple_of(t * TQ, TQ), TQ)
        if not first:
            old_top = old_ref[136:137, at]
            top = jnp.maximum(old_top, top)
        total = None
        for j in range(0, len(pieces), 2):
            p = jnp.exp(s[384 * j : 384 * (j + 2), :] - top).astype(BF)
            v = jnp.concatenate(
                [kv_refs[w][row + 128 * i : row + 128 * (i + 1), :] for w, _, row in pieces[j : j + 2] for i in range(3)],
                axis=1,
            )
            ones = jnp.ones((16, 768), BF)
            d = jnp.dot(jnp.concatenate([v, ones], axis=0), p, preferred_element_type=F32)
            total = d if total is None else total + d
        total = total[:136]
        if not first:
            total = old_ref[0:136, at] * jnp.exp(old_top - top) + total
        new_ref[0:136, at] = total
        new_ref[136:144, at] = jnp.broadcast_to(top, (8, TQ))

    top = scores(0, sa)
    for part in range(parts):

        def body(i, top):
            t = 2 * i
            base = each * part
            top_b = scores(base + t + 1, sb)
            add(t, sa, top, old_refs[part], new_refs[part])
            top_a = scores(jnp.minimum(base + t + 2, tiles - 1), sa)
            add(t + 1, sb, top_b, old_refs[part], new_refs[part])
            return top_a

        top = lax.fori_loop(0, each // 2, body, top)


def attend(q, arrays, pieces, states, parts=2, start=0):
    first = states is None
    n = 1536 * parts
    keys = 384 * len(pieces)
    args = [q, *arrays] + ([] if first else list(states))
    return pl.pallas_call(
        functools.partial(attend_body, pieces=pieces, first=first, parts=parts, start=start),
        in_specs=whole(len(args)),
        out_specs=whole(parts),
        out_shape=[jax.ShapeDtypeStruct((144, n // parts), F32)] * parts,
        scratch_shapes=[pltpu.VMEM((keys, TQ), F32)] * 2,
        input_output_aliases={} if first or parts == 1 else {len(args) - parts + i: i for i in range(parts)},
        compiler_params=pltpu.CompilerParams(vmem_limit_bytes=16 * 2**20),
        cost_estimate=pl.CostEstimate(flops=8 * 256 * n * keys, bytes_accessed=2**22, transcendentals=n * keys),
        name="attend",
    )(*args)


def pack_body(gate_hbm, up_hbm, down_hbm, out_ref, gate_ref, up_ref, down_ref, sems):
    copies = [
        pltpu.make_async_copy(a, b, sems.at[i])
        for i, (a, b) in enumerate(((gate_hbm, gate_ref), (up_hbm, up_ref), (down_hbm, down_ref)))
    ]
    for copy in copies:
        copy.start()
    for copy in copies:
        copy.wait()
    for i, (a, b) in enumerate(((0, 256), (256, 512), (512, 640))):
        out_ref[:, 512 * i : 512 * i + b - a] = gate_ref[:, a:b]
        out_ref[:, 512 * i + b - a : 512 * i + 2 * (b - a)] = up_ref[:, a:b]
    tails = [r[:, 640:704].astype(F32) for r in (gate_ref, up_ref)]
    out_ref[:, 1280:1408] = jnp.concatenate(tails, axis=1).astype(BF)
    out_ref[:, 1408:2048] = down_ref[:, 0:640]
    last = jnp.concatenate([down_ref[:, 640:704].astype(F32), jnp.zeros((64, 64), F32)], axis=1)
    out_ref[:, 2048:2176] = last.astype(BF)


def pack(gate, up, down):
    return pl.pallas_call(
        pack_body,
        in_specs=[pl.BlockSpec(memory_space=pltpu.HBM)] * 3,
        out_specs=pl.BlockSpec(memory_space=pltpu.VMEM),
        out_shape=jax.ShapeDtypeStruct((64, 2176), BF),
        scratch_shapes=[
            pltpu.VMEM((64, 704), BF),
            pltpu.VMEM((64, 704), BF),
            pltpu.VMEM((64, 704), BF),
            pltpu.SemaphoreType.DMA((3,)),
        ],
        compiler_params=pltpu.CompilerParams(vmem_limit_bytes=63 * 2**20),
        cost_estimate=pl.CostEstimate(flops=10**7, bytes_accessed=2**19, transcendentals=0),
        name="pack",
    )(gate, up, down)


def small(body, shapes, scalars, *args):
    alone = not isinstance(shapes, list)
    return pl.pallas_call(
        body,
        in_specs=[pl.BlockSpec(memory_space=pltpu.SMEM)] * scalars + whole(len(args) - scalars),
        out_specs=pl.BlockSpec(memory_space=pltpu.VMEM) if alone else whole(len(shapes)),
        out_shape=jax.ShapeDtypeStruct(*shapes) if alone else [jax.ShapeDtypeStruct(*sh) for sh in shapes],
        compiler_params=pltpu.CompilerParams(vmem_limit_bytes=8 * 2**20),
        cost_estimate=pl.CostEstimate(flops=10**7, bytes_accessed=2**20, transcendentals=0),
    )(*args)


def send_body(c_ref, q_hbm, k_hbm, v_hbm, own_ref, out_ref, q_ref, k_ref, v_ref, sems):
    pairs = ((q_hbm, q_ref), (k_hbm, k_ref), (v_hbm, v_ref))
    copies = [pltpu.make_async_copy(a, b, sems.at[i]) for i, (a, b) in enumerate(pairs)]
    for copy in copies:
        copy.start()
    for copy in copies:
        copy.wait()
    c = c_ref[0]
    for sub, to_ref in ((c, own_ref), (1 - c, out_ref)):
        for x in range(4):
            to_ref[48 * x : 48 * (x + 1), :] = q_ref[pl.ds(pl.multiple_of(96 * x + 48 * sub, 48), 48), :]
        at = pl.ds(pl.multiple_of(192 * sub, 192), 192)
        to_ref[192:384, :] = k_ref[at, :]
        to_ref[384:576, :] = v_ref[at, :]


def send(core, q, k, v):
    half = jax.ShapeDtypeStruct((576, 256), BF)
    return pl.pallas_call(
        send_body,
        in_specs=[pl.BlockSpec(memory_space=pltpu.SMEM)] + [pl.BlockSpec(memory_space=pltpu.HBM)] * 3,
        out_specs=whole(2),
        out_shape=[half, half],
        scratch_shapes=[pltpu.VMEM((384, 256), BF)] * 3 + [pltpu.SemaphoreType.DMA((3,))],
        compiler_params=pltpu.CompilerParams(vmem_limit_bytes=63 * 2**20),
        cost_estimate=pl.CostEstimate(flops=10**7, bytes_accessed=2**20, transcendentals=0),
        name="send",
    )(core, q, k, v)


def heads_body(c_ref, own_ref, got_ref, out_ref):
    c = c_ref[0]
    for j in range(2):
        lanes = slice(128 * j, 128 * (j + 1))
        out_ref[2 * c + j] = own_ref[:, lanes]
        out_ref[2 - 2 * c + j] = got_ref[:, lanes]


def block_body(head_ref, block_ref, q_ref):
    for i in range(4):
        at = 768 * (i // 2) + 192 * (i % 2)
        block_ref[at : at + 192, :] = head_ref[i, 192:384, :]
        q_ref[192 * i : 192 * (i + 1), :] = head_ref[i, 0:192, :]
    values = jnp.concatenate([head_ref[i, 384:576, :] for i in range(4)], axis=0)
    for i in range(6):
        at = 768 * (i // 3) + 384 + 128 * (i % 3)
        block_ref[at : at + 128, :] = values[128 * i : 128 * (i + 1), :].T


def queries_body(other_ref, own_ref, out_ref):
    lane = lax.broadcasted_iota(jnp.int32, (768, 128), 1)
    for i, ref in enumerate((other_ref, own_ref)):
        rows = ref[...].astype(F32) * 0.125
        out_ref[1536 * i : 1536 * i + 768, :] = jnp.where(lane < 64, rows, 0.0).astype(BF)
        out_ref[1536 * i + 768 : 1536 * (i + 1), :] = jnp.where(lane < 64, 0.0, rows).astype(BF)


def carry_body(w_ref, r_ref, out_ref):
    out_ref[0:256, :] = w_ref[...]
    out_ref[256:304, :] = r_ref[...]


def finish_body(y_ref, c_ref, lam_ref, lam_got_ref, mine_ref, other_ref, gain_ref, out_ref):
    n = 768
    y, c = y_ref[0], c_ref[0]
    lam = jnp.where(c == y // 2, lam_ref[y % 2], lam_got_ref[y % 2])
    gain = gain_ref[...]
    for t in range(n // 128):
        maps = []
        for comp in range(2):
            at = slice(n * comp + 128 * t, n * comp + 128 * (t + 1))
            m0, m1 = mine_ref[136:137, at], other_ref[136:137, at]
            top = jnp.maximum(m0, m1)
            w0, w1 = jnp.exp(m0 - top), jnp.exp(m1 - top)
            total = mine_ref[128:129, at] * w0 + other_ref[128:129, at] * w1
            maps.append((mine_ref[0:128, at] * w0 + other_ref[0:128, at] * w1) / total)
        mixed = maps[0] - lam * maps[1]
        scale = lax.rsqrt(jnp.mean(mixed * mixed, axis=0, keepdims=True) + 1e-06)
        rows = ((mixed * scale).T * gain).astype(BF)
        for at in (128 * t, 128 * t + 64):
            for x in range(4):
                out_ref[at // 192, x, at % 192 : at % 192 + 64, :] = rows[at - 128 * t : at - 128 * t + 64]


def finish(y, c, lam, lam_got, mine, other, gain):
    return pl.pallas_call(
        finish_body,
        in_specs=[pl.BlockSpec(memory_space=pltpu.SMEM)] * 4 + whole(3),
        out_specs=pl.BlockSpec(memory_space=pltpu.VMEM),
        out_shape=jax.ShapeDtypeStruct((Y, X, 192, 128), BF),
        compiler_params=pltpu.CompilerParams(vmem_limit_bytes=8 * 2**20),
        cost_estimate=pl.CostEstimate(flops=10**8, bytes_accessed=2**21, transcendentals=0),
        name="finish",
    )(y, c, lam, lam_got, mine, other, gain)


def layer_body(x_ref, c_ref, *refs):
    g_hbm, gain_hbm, *hbm = refs[:10]
    w_hbm, out_hbm, own_hbm, g_ref, gain_ref, out_ref, own_ref, po, wf, acc, xn, hid, sems = refs[10:]
    x, c = x_ref[0], c_ref[0]
    copies = []
    for half in range(2):
        lanes = slice(1024 * half, 1024 * (half + 1))
        for i, ref in enumerate(hbm):
            copies.append(pltpu.make_async_copy(ref.at[:, lanes], po.at[i, :, lanes], sems.at[8 * half + i]))
    chunks = [(c2, a, b) for c2 in range(2) for a, b in ((0, 512), (512, 1024), (1024, 1408))]
    views = [(slice(None), c2, slice(None), slice(a, b)) for c2, a, b in chunks]
    views += [(slice(16 * i, 16 * (i + 1)), slice(None), slice(None), slice(1408, 2176)) for i in range(2)]
    streams = [pltpu.make_async_copy(w_hbm.at[v], wf.at[v], sems.at[16 + i]) for i, v in enumerate(views)]
    rows_in = pltpu.make_async_copy(g_hbm, g_ref, sems.at[24])
    gain_in = pltpu.make_async_copy(gain_hbm, gain_ref, sems.at[25])
    for copy in [rows_in, gain_in, *copies, *streams]:
        copy.start()
    rows_in.wait()
    gain_in.wait()

    blocks = []
    for k in range(8):
        xk = lax.rem(x + 4 + (0, -1, 1, 2)[k // 2], 4)
        ck = c if k % 2 == 0 else 1 - c
        blocks.append(jnp.concatenate([g_ref[2 * ck, xk], g_ref[2 * ck + 1, xk]], axis=1))
    for half in range(2):
        for copy in copies[8 * half : 8 * half + 8]:
            copy.wait()
        for n in range(2):
            lanes = slice(1024 * half + 512 * n, 1024 * half + 512 * (n + 1))
            total = None
            for k, a in enumerate(blocks):
                d = jnp.dot(a, po[k, 0:256, lanes], preferred_element_type=F32)
                total = d if total is None else total + d
            acc[:, lanes] = total
    for k, step in ((0, 0), (2, -1), (4, 1), (6, 2)):
        at = pl.ds(pl.multiple_of(48 * lax.rem(x + 4 + step, 4), 16), 48)
        acc[at, :] += po[k, 256:304, :].astype(F32)
    own_ref[...] = acc[pl.ds(pl.multiple_of(48 * x, 16), 48), :]
    own_out = pltpu.make_async_copy(own_ref, own_hbm, sems.at[26])
    own_out.start()
    gain = gain_ref[...]
    for i in range(6):
        rows = acc[32 * i : 32 * (i + 1), :]
        scale = lax.rsqrt(jnp.mean(rows * rows, axis=1, keepdims=True) + 1e-06)
        xn[32 * i : 32 * (i + 1), :] = (rows * scale * gain).astype(BF)

    for i, (c2, a, b) in enumerate(chunks):
        streams[i].wait()
        gu = jnp.dot(xn[...], wf[:, c2, :, a:b].reshape(2048, b - a), preferred_element_type=F32)
        n = 256 if b - a == 512 else 128
        at = 768 * c2 + a // 2
        hid[:, at : at + n] = (jax.nn.silu(gu[:, 0:n]) * gu[:, n : 2 * n]).astype(BF)
        if n == 128:
            tail = gu[:, 256:384]
            both = jax.nn.silu(tail) * pltpu.roll(tail, 64, 1)
            lane = lax.broadcasted_iota(jnp.int32, both.shape, 1)
            hid[:, at + 128 : at + 256] = jnp.where(lane < 64, both, 0.0).astype(BF)
    outs = []
    for half in range(2):
        streams[6 + half].wait()

        @pl.loop(2 * half, 2 * half + 2)
        def _(m):
            for part in range(2):
                total = None
                for c2 in range(2):
                    w = wf[pl.ds(8 * m + 4 * part, 4), c2, :, 1408:2176].reshape(256, 768)
                    d = lax.dot_general(
                        hid[:, 768 * c2 : 768 * (c2 + 1)], w, (((1,), (1,)), ((), ())), preferred_element_type=F32
                    )
                    total = d if total is None else total + d
                out_ref[:, pl.ds(pl.multiple_of(512 * m + 256 * part, 256), 256)] = total.astype(BF)

        lanes = slice(1024 * half, 1024 * (half + 1))
        outs.append(pltpu.make_async_copy(out_ref.at[:, lanes], out_hbm.at[:, lanes], sems.at[27 + half]))
        outs[half].start()
    for copy in [own_out, *outs]:
        copy.wait()


def layer(x, c, g, gain, blocks, w):
    return pl.pallas_call(
        layer_body,
        in_specs=[pl.BlockSpec(memory_space=pltpu.SMEM)] * 2 + [pl.BlockSpec(memory_space=pltpu.HBM)] * 11,
        out_specs=[pl.BlockSpec(memory_space=pltpu.HBM)] * 2,
        out_shape=[jax.ShapeDtypeStruct((192, 2048), BF), jax.ShapeDtypeStruct((48, 2048), F32)],
        scratch_shapes=[
            pltpu.VMEM(g.shape, BF),
            pltpu.VMEM(gain.shape, F32),
            pltpu.VMEM((192, 2048), BF),
            pltpu.VMEM((48, 2048), F32),
            pltpu.VMEM((8, 304, 2048), BF),
            pltpu.VMEM(w.shape, BF),
            pltpu.VMEM((192, 2048), F32),
            pltpu.VMEM((192, 2048), BF),
            pltpu.VMEM((192, 1536), BF),
            pltpu.SemaphoreType.DMA((29,)),
        ],
        compiler_params=pltpu.CompilerParams(vmem_limit_bytes=62 * 2**20),
        cost_estimate=pl.CostEstimate(flops=8 * 192 * 2048 * 2048, bytes_accessed=28 * 2**20, transcendentals=0),
        name="layer",
    )(x, c, g, gain, *blocks, w)


def swap(v):
    return lax.ppermute(v, "c", [(0, 1), (1, 0)])


def around(v, step, axis="z", n=Z):
    return lax.ppermute(v, axis, [(i, (i + step) % n) for i in range(n)])


def exchange(v, axis):
    return lax.all_to_all(v, axis, split_axis=0, concat_axis=0, tiled=True)


def inner(residual, queries, keys, values, mix_lambda, head_gain, out_weight, norm_gain, gate, up, down):
    x, y, c = lax.axis_index("x"), lax.axis_index("y"), lax.axis_index("c")

    packed = pack(gate, up, down.T)
    weights = lax.all_gather(packed, ("z", "y", "c"), axis=0, tiled=False).reshape(32, 2, 64, 2176)

    core, x, y = c.reshape(1), x.reshape(1), y.reshape(1)
    after = lax.optimization_barrier
    kept, sent = send(core, queries, keys, values)
    heads = small(heads_body, ((Y, 576, 128), BF), 1, core, kept, swap(sent))
    head = exchange(heads, "y")

    heads, out_weight, residual = after((heads, out_weight, residual))
    carry = small(carry_body, ((304, 2048), BF), 0, out_weight, residual)
    from_left, from_right = around(carry, 1, "x", X), around(carry, -1, "x", X)
    carry_c = swap(carry)

    block, q_own = small(block_body, [((1536, 128), BF), ((768, 128), BF)], 0, head)
    right, left = around(block, 1), around(block, -1)
    q_other = swap(q_own)
    lam_got = swap(mix_lambda)
    q_all = small(queries_body, ((3072, 128), BF), 0, q_other, q_own)
    q_all, lam_got = after((q_all, lam_got))

    one = [(0, 0, 384), (0, 768, 1152)]
    two = one + [(1, 0, 384), (1, 768, 1152)]
    states = attend(q_all, [block], one, None)
    states, right, left = after((states, right, left))
    right2, left2 = around(right, 1), around(left, -1)
    states = attend(q_all, [right, left], two, states)
    states, right2, left2 = after((states, right2, left2))
    right3, left3 = around(right2, 1), around(left2, -1)
    states, from_left, from_right, carry_c = after((states, from_left, from_right, carry_c))
    far = around(from_left, 1, "x", X)
    left_c, right_c = swap(from_left), swap(from_right)
    states = attend(q_all, [right2, left2], two, states)
    states, right3, left3 = after((states, right3, left3))
    last_r, last_l = around(right3[:768], 1), around(left3[768:], -1)
    states = attend(q_all, [right3, left3], two, states)
    states, last_r, last_l, left_c, right_c = after((states, last_r, last_l, left_c, right_c))
    ends = [(0, 0, 384), (1, 0, 384)]
    (theirs,) = attend(q_all, [last_r, last_l], ends, states[:1], 1)
    other = swap(theirs)
    (own,) = attend(q_all, [last_r, last_l], ends, states[1:], 1, 6)
    own, far = after((own, far))
    far_c = swap(far)

    attended = finish(y, core, mix_lambda, lam_got, own, other, head_gain.reshape(1, 128)).reshape(Y * X, 192, 128)
    spread = exchange(attended, ("y", "x")).reshape(Y, X, 192, 128)
    blocks = [carry, carry_c, from_left, left_c, from_right, right_c, far, far_c]
    spread, weights = after((spread, weights))
    mixed, after_mix = layer(x, core, spread, norm_gain.reshape(1, 2048), blocks, weights)
    mixed = exchange(mixed.reshape(X, 48, 2048), "x").astype(F32).sum(axis=0)
    return (after_mix + 0.5 * mixed).astype(BF)


def solution(mesh):
    split = Mesh(mesh.devices.reshape(Z, Y, X, C), ("z", "y", "x", "c"))
    sp, tp = ("z", "y"), ("x", "c")
    return jax.shard_map(
        inner,
        mesh=split,
        in_specs=(
            P(("z", "y", "x", "c"), None),
            P(sp, tp),
            P(sp, tp),
            P(sp, tp),
            P(tp),
            P(),
            P(tp, None),
            P(),
            P(sp, tp),
            P(sp, tp),
            P(tp, sp),
        ),
        out_specs=P(("z", "y", "x", "c"), None),
        check_vma=False,
    )
```

```python
import functools

import jax
import jax.numpy as jnp
from jax import lax
from jax.experimental import pallas as pl
from jax.experimental.pallas import tpu as pltpu
from jax.sharding import Mesh, PartitionSpec as P


BF = jnp.bfloat16
F32 = jnp.float32
Z, Y, X, C = 8, 4, 4, 2
TQ = 256


def whole(n):
    return [pl.BlockSpec(memory_space=pltpu.VMEM)] * n


def attend_body(*refs, pieces, first, parts, start):
    count = 1 + max(p[0] for p in pieces)
    q_ref, kv_refs = refs[0], refs[1 : 1 + count]
    old_refs = [None] * parts if first else refs[1 + count : 1 + count + parts]
    new_refs = refs[-2 - parts : -2]
    sa, sb = refs[-2:]
    each = new_refs[0].shape[1] // TQ
    tiles = each * parts

    def scores(t, s):
        q = q_ref[pl.ds(pl.multiple_of((start + t) * TQ, TQ), TQ), :]
        top = None
        for j, (which, row, _) in enumerate(pieces):
            d = lax.dot_general(
                kv_refs[which][row : row + 384, :], q, (((1,), (1,)), ((), ())), preferred_element_type=F32
            )
            s[384 * j : 384 * (j + 1), :] = d
            m = jnp.max(d.reshape(48, 8, TQ), axis=0)
            top = m if top is None else jnp.maximum(top, m)
        return jnp.max(top, axis=0, keepdims=True)

    def add(t, s, top, old_ref, new_ref):
        at = pl.ds(pl.multiple_of(t * TQ, TQ), TQ)
        if not first:
            old_top = old_ref[136:137, at]
            top = jnp.maximum(old_top, top)
        total = None
        for j in range(0, len(pieces), 2):
            p = jnp.exp(s[384 * j : 384 * (j + 2), :] - top).astype(BF)
            v = jnp.concatenate(
                [kv_refs[w][row + 128 * i : row + 128 * (i + 1), :] for w, _, row in pieces[j : j + 2] for i in range(3)],
                axis=1,
            )
            ones = jnp.ones((16, 768), BF)
            d = jnp.dot(jnp.concatenate([v, ones], axis=0), p, preferred_element_type=F32)
            total = d if total is None else total + d
        total = total[:136]
        if not first:
            total = old_ref[0:136, at] * jnp.exp(old_top - top) + total
        new_ref[0:136, at] = total
        new_ref[136:144, at] = jnp.broadcast_to(top, (8, TQ))

    top = scores(0, sa)
    for part in range(parts):

        def body(i, top):
            t = 2 * i
            base = each * part
            top_b = scores(base + t + 1, sb)
            add(t, sa, top, old_refs[part], new_refs[part])
            top_a = scores(jnp.minimum(base + t + 2, tiles - 1), sa)
            add(t + 1, sb, top_b, old_refs[part], new_refs[part])
            return top_a

        top = lax.fori_loop(0, each // 2, body, top)


def attend(q, arrays, pieces, states, parts=2, start=0):
    first = states is None
    n = 1536 * parts
    keys = 384 * len(pieces)
    args = [q, *arrays] + ([] if first else list(states))
    return pl.pallas_call(
        functools.partial(attend_body, pieces=pieces, first=first, parts=parts, start=start),
        in_specs=whole(len(args)),
        out_specs=whole(parts),
        out_shape=[jax.ShapeDtypeStruct((144, n // parts), F32)] * parts,
        scratch_shapes=[pltpu.VMEM((keys, TQ), F32)] * 2,
        input_output_aliases={} if first or parts == 1 else {len(args) - parts + i: i for i in range(parts)},
        compiler_params=pltpu.CompilerParams(vmem_limit_bytes=16 * 2**20),
        cost_estimate=pl.CostEstimate(flops=8 * 256 * n * keys, bytes_accessed=2**22, transcendentals=n * keys),
        name="attend",
    )(*args)


def pack_body(gate_hbm, up_hbm, down_hbm, out_ref, gate_ref, up_ref, down_ref, sems):
    copies = [
        pltpu.make_async_copy(a, b, sems.at[i])
        for i, (a, b) in enumerate(((gate_hbm, gate_ref), (up_hbm, up_ref), (down_hbm, down_ref)))
    ]
    for copy in copies:
        copy.start()
    for copy in copies:
        copy.wait()
    for i, (a, b) in enumerate(((0, 256), (256, 512), (512, 640))):
        out_ref[:, 512 * i : 512 * i + b - a] = gate_ref[:, a:b]
        out_ref[:, 512 * i + b - a : 512 * i + 2 * (b - a)] = up_ref[:, a:b]
    tails = [r[:, 640:704].astype(F32) for r in (gate_ref, up_ref)]
    out_ref[:, 1280:1408] = jnp.concatenate(tails, axis=1).astype(BF)
    out_ref[:, 1408:2048] = down_ref[:, 0:640]
    last = jnp.concatenate([down_ref[:, 640:704].astype(F32), jnp.zeros((64, 64), F32)], axis=1)
    out_ref[:, 2048:2176] = last.astype(BF)


def pack(gate, up, down):
    return pl.pallas_call(
        pack_body,
        in_specs=[pl.BlockSpec(memory_space=pltpu.HBM)] * 3,
        out_specs=pl.BlockSpec(memory_space=pltpu.VMEM),
        out_shape=jax.ShapeDtypeStruct((64, 2176), BF),
        scratch_shapes=[
            pltpu.VMEM((64, 704), BF),
            pltpu.VMEM((64, 704), BF),
            pltpu.VMEM((64, 704), BF),
            pltpu.SemaphoreType.DMA((3,)),
        ],
        compiler_params=pltpu.CompilerParams(vmem_limit_bytes=63 * 2**20),
        cost_estimate=pl.CostEstimate(flops=10**7, bytes_accessed=2**19, transcendentals=0),
        name="pack",
    )(gate, up, down)


def small(body, shapes, scalars, *args):
    alone = not isinstance(shapes, list)
    return pl.pallas_call(
        body,
        in_specs=[pl.BlockSpec(memory_space=pltpu.SMEM)] * scalars + whole(len(args) - scalars),
        out_specs=pl.BlockSpec(memory_space=pltpu.VMEM) if alone else whole(len(shapes)),
        out_shape=jax.ShapeDtypeStruct(*shapes) if alone else [jax.ShapeDtypeStruct(*sh) for sh in shapes],
        compiler_params=pltpu.CompilerParams(vmem_limit_bytes=8 * 2**20),
        cost_estimate=pl.CostEstimate(flops=10**7, bytes_accessed=2**20, transcendentals=0),
    )(*args)


def send_body(c_ref, q_hbm, k_hbm, v_hbm, own_ref, out_ref, q_ref, k_ref, v_ref, sems):
    pairs = ((q_hbm, q_ref), (k_hbm, k_ref), (v_hbm, v_ref))
    copies = [pltpu.make_async_copy(a, b, sems.at[i]) for i, (a, b) in enumerate(pairs)]
    for copy in copies:
        copy.start()
    for copy in copies:
        copy.wait()
    c = c_ref[0]
    for sub, to_ref in ((c, own_ref), (1 - c, out_ref)):
        for x in range(4):
            to_ref[48 * x : 48 * (x + 1), :] = q_ref[pl.ds(pl.multiple_of(96 * x + 48 * sub, 48), 48), :]
        at = pl.ds(pl.multiple_of(192 * sub, 192), 192)
        to_ref[192:384, :] = k_ref[at, :]
        to_ref[384:576, :] = v_ref[at, :]


def send(core, q, k, v):
    half = jax.ShapeDtypeStruct((576, 256), BF)
    return pl.pallas_call(
        send_body,
        in_specs=[pl.BlockSpec(memory_space=pltpu.SMEM)] + [pl.BlockSpec(memory_space=pltpu.HBM)] * 3,
        out_specs=whole(2),
        out_shape=[half, half],
        scratch_shapes=[pltpu.VMEM((384, 256), BF)] * 3 + [pltpu.SemaphoreType.DMA((3,))],
        compiler_params=pltpu.CompilerParams(vmem_limit_bytes=63 * 2**20),
        cost_estimate=pl.CostEstimate(flops=10**7, bytes_accessed=2**20, transcendentals=0),
        name="send",
    )(core, q, k, v)


def heads_body(c_ref, own_ref, got_ref, out_ref):
    c = c_ref[0]
    for j in range(2):
        lanes = slice(128 * j, 128 * (j + 1))
        out_ref[2 * c + j] = own_ref[:, lanes]
        out_ref[2 - 2 * c + j] = got_ref[:, lanes]


def block_body(head_ref, block_ref, q_ref):
    for i in range(4):
        at = 768 * (i // 2) + 192 * (i % 2)
        block_ref[at : at + 192, :] = head_ref[i, 192:384, :]
        q_ref[192 * i : 192 * (i + 1), :] = head_ref[i, 0:192, :]
    values = jnp.concatenate([head_ref[i, 384:576, :] for i in range(4)], axis=0)
    for i in range(6):
        at = 768 * (i // 3) + 384 + 128 * (i % 3)
        block_ref[at : at + 128, :] = values[128 * i : 128 * (i + 1), :].T


def queries_body(other_ref, own_ref, out_ref):
    lane = lax.broadcasted_iota(jnp.int32, (768, 128), 1)
    for i, ref in enumerate((other_ref, own_ref)):
        rows = ref[...].astype(F32) * 0.125
        out_ref[1536 * i : 1536 * i + 768, :] = jnp.where(lane < 64, rows, 0.0).astype(BF)
        out_ref[1536 * i + 768 : 1536 * (i + 1), :] = jnp.where(lane < 64, 0.0, rows).astype(BF)


def carry_body(w_ref, r_ref, out_ref):
    out_ref[0:256, :] = w_ref[...]
    out_ref[256:304, :] = r_ref[...]


def finish_body(y_ref, c_ref, lam_ref, lam_got_ref, mine_ref, other_ref, gain_ref, out_ref):
    n = 768
    y, c = y_ref[0], c_ref[0]
    lam = jnp.where(c == y // 2, lam_ref[y % 2], lam_got_ref[y % 2])
    gain = gain_ref[...]
    for t in range(n // 128):
        maps = []
        for comp in range(2):
            at = slice(n * comp + 128 * t, n * comp + 128 * (t + 1))
            m0, m1 = mine_ref[136:137, at], other_ref[136:137, at]
            top = jnp.maximum(m0, m1)
            w0, w1 = jnp.exp(m0 - top), jnp.exp(m1 - top)
            total = mine_ref[128:129, at] * w0 + other_ref[128:129, at] * w1
            maps.append((mine_ref[0:128, at] * w0 + other_ref[0:128, at] * w1) / total)
        mixed = maps[0] - lam * maps[1]
        scale = lax.rsqrt(jnp.mean(mixed * mixed, axis=0, keepdims=True) + 1e-06)
        rows = ((mixed * scale).T * gain).astype(BF)
        for at in (128 * t, 128 * t + 64):
            for x in range(4):
                out_ref[at // 192, x, at % 192 : at % 192 + 64, :] = rows[at - 128 * t : at - 128 * t + 64]


def finish(y, c, lam, lam_got, mine, other, gain):
    return pl.pallas_call(
        finish_body,
        in_specs=[pl.BlockSpec(memory_space=pltpu.SMEM)] * 4 + whole(3),
        out_specs=pl.BlockSpec(memory_space=pltpu.VMEM),
        out_shape=jax.ShapeDtypeStruct((Y, X, 192, 128), BF),
        compiler_params=pltpu.CompilerParams(vmem_limit_bytes=8 * 2**20),
        cost_estimate=pl.CostEstimate(flops=10**8, bytes_accessed=2**21, transcendentals=0),
        name="finish",
    )(y, c, lam, lam_got, mine, other, gain)


def layer_body(x_ref, c_ref, *refs):
    g_hbm, gain_hbm, *hbm = refs[:10]
    w_hbm, *out_hbm, own_hbm = refs[10:15]
    g_ref, gain_ref, out_ref, own_ref, po, wf, acc, xn, hid, sems = refs[15:]
    x, c = x_ref[0], c_ref[0]
    copies = []
    for half in range(2):
        lanes = slice(1024 * half, 1024 * (half + 1))
        for i, ref in enumerate(hbm):
            copies.append(pltpu.make_async_copy(ref.at[:, lanes], po.at[i, :, lanes], sems.at[8 * half + i]))
    chunks = [(c2, a, b) for c2 in range(2) for a, b in ((0, 512), (512, 1024), (1024, 1408))]
    views = [(slice(None), c2, slice(None), slice(a, b)) for c2, a, b in chunks]
    views += [(slice(16 * i, 16 * (i + 1)), slice(None), slice(None), slice(1408, 2176)) for i in range(2)]
    streams = [pltpu.make_async_copy(w_hbm.at[v], wf.at[v], sems.at[16 + i]) for i, v in enumerate(views)]
    rows_in = pltpu.make_async_copy(g_hbm, g_ref, sems.at[24])
    gain_in = pltpu.make_async_copy(gain_hbm, gain_ref, sems.at[25])
    for copy in [rows_in, gain_in, *copies, *streams]:
        copy.start()
    rows_in.wait()
    gain_in.wait()

    blocks = []
    for k in range(8):
        xk = lax.rem(x + 4 + (0, -1, 1, 2)[k // 2], 4)
        ck = c if k % 2 == 0 else 1 - c
        blocks.append(jnp.concatenate([g_ref[2 * ck, xk], g_ref[2 * ck + 1, xk]], axis=1))
    for half in range(2):
        for copy in copies[8 * half : 8 * half + 8]:
            copy.wait()
        for n in range(2):
            lanes = slice(1024 * half + 512 * n, 1024 * half + 512 * (n + 1))
            total = None
            for k, a in enumerate(blocks):
                d = jnp.dot(a, po[k, 0:256, lanes], preferred_element_type=F32)
                total = d if total is None else total + d
            acc[:, lanes] = total
    for k, step in ((0, 0), (2, -1), (4, 1), (6, 2)):
        at = pl.ds(pl.multiple_of(48 * lax.rem(x + 4 + step, 4), 16), 48)
        acc[at, :] += po[k, 256:304, :].astype(F32)
    own_ref[...] = acc[pl.ds(pl.multiple_of(48 * x, 16), 48), :]
    gain = gain_ref[...]
    for i in range(6):
        rows = acc[32 * i : 32 * (i + 1), :]
        scale = lax.rsqrt(jnp.mean(rows * rows, axis=1, keepdims=True) + 1e-06)
        xn[32 * i : 32 * (i + 1), :] = (rows * scale * gain).astype(BF)

    for i, (c2, a, b) in enumerate(chunks):
        streams[i].wait()
        gu = jnp.dot(xn[...], wf[:, c2, :, a:b].reshape(2048, b - a), preferred_element_type=F32)
        n = 256 if b - a == 512 else 128
        at = 768 * c2 + a // 2
        hid[:, at : at + n] = (jax.nn.silu(gu[:, 0:n]) * gu[:, n : 2 * n]).astype(BF)
        if n == 128:
            tail = gu[:, 256:384]
            both = jax.nn.silu(tail) * pltpu.roll(tail, 64, 1)
            lane = lax.broadcasted_iota(jnp.int32, both.shape, 1)
            hid[:, at + 128 : at + 256] = jnp.where(lane < 64, both, 0.0).astype(BF)
    outs = []
    for half in range(2):
        streams[6 + half].wait()

        @pl.loop(2 * half, 2 * half + 2)
        def _(m):
            for part in range(2):
                total = None
                for c2 in range(2):
                    w = wf[pl.ds(8 * m + 4 * part, 4), c2, :, 1408:2176].reshape(256, 768)
                    d = lax.dot_general(
                        hid[:, 768 * c2 : 768 * (c2 + 1)], w, (((1,), (1,)), ((), ())), preferred_element_type=F32
                    )
                    total = d if total is None else total + d
                out_ref[:, pl.ds(pl.multiple_of(512 * m + 256 * part, 256), 256)] = total.astype(BF)

        lanes = slice(1024 * half, 1024 * (half + 1))
        for i, step in enumerate((2, 1, -1)):
            at = pl.ds(pl.multiple_of(48 * lax.rem(x + 4 + step, 4), 16), 48)
            outs.append(pltpu.make_async_copy(out_ref.at[at, lanes], out_hbm[i].at[:, lanes], sems.at[26 + 3 * half + i]))
            outs[-1].start()
        rows = out_ref[pl.ds(pl.multiple_of(48 * x, 16), 48), lanes]
        own_ref[:, lanes] += 0.5 * rows.astype(F32)
        outs.append(pltpu.make_async_copy(own_ref.at[:, lanes], own_hbm.at[:, lanes], sems.at[32 + half]))
        outs[-1].start()
    for copy in outs:
        copy.wait()


def layer(x, c, g, gain, blocks, w):
    return pl.pallas_call(
        layer_body,
        in_specs=[pl.BlockSpec(memory_space=pltpu.SMEM)] * 2 + [pl.BlockSpec(memory_space=pltpu.HBM)] * 11,
        out_specs=[pl.BlockSpec(memory_space=pltpu.HBM)] * 4,
        out_shape=[jax.ShapeDtypeStruct((48, 2048), BF)] * 3 + [jax.ShapeDtypeStruct((48, 2048), F32)],
        scratch_shapes=[
            pltpu.VMEM(g.shape, BF),
            pltpu.VMEM(gain.shape, F32),
            pltpu.VMEM((192, 2048), BF),
            pltpu.VMEM((48, 2048), F32),
            pltpu.VMEM((8, 304, 2048), BF),
            pltpu.VMEM(w.shape, BF),
            pltpu.VMEM((192, 2048), F32),
            pltpu.VMEM((192, 2048), BF),
            pltpu.VMEM((192, 1536), BF),
            pltpu.SemaphoreType.DMA((34,)),
        ],
        compiler_params=pltpu.CompilerParams(vmem_limit_bytes=62 * 2**20),
        cost_estimate=pl.CostEstimate(flops=8 * 192 * 2048 * 2048, bytes_accessed=28 * 2**20, transcendentals=0),
        name="layer",
    )(x, c, g, gain, *blocks, w)


def swap(v):
    return lax.ppermute(v, "c", [(0, 1), (1, 0)])


def around(v, step, axis="z", n=Z):
    return lax.ppermute(v, axis, [(i, (i + step) % n) for i in range(n)])


def exchange(v, axis):
    return lax.all_to_all(v, axis, split_axis=0, concat_axis=0, tiled=True)


def inner(residual, queries, keys, values, mix_lambda, head_gain, out_weight, norm_gain, gate, up, down):
    x, y, c = lax.axis_index("x"), lax.axis_index("y"), lax.axis_index("c")

    packed = pack(gate, up, down.T)
    weights = lax.all_gather(packed, ("z", "y", "c"), axis=0, tiled=False).reshape(32, 2, 64, 2176)

    core, x, y = c.reshape(1), x.reshape(1), y.reshape(1)
    after = lax.optimization_barrier
    kept, sent = send(core, queries, keys, values)
    heads = small(heads_body, ((Y, 576, 128), BF), 1, core, kept, swap(sent))
    head = exchange(heads, "y")

    heads, out_weight, residual = after((heads, out_weight, residual))
    carry = small(carry_body, ((304, 2048), BF), 0, out_weight, residual)
    from_left, from_right = around(carry, 1, "x", X), around(carry, -1, "x", X)
    carry_c = swap(carry)

    block, q_own = small(block_body, [((1536, 128), BF), ((768, 128), BF)], 0, head)
    right, left = around(block, 1), around(block, -1)
    q_other = swap(q_own)
    lam_got = swap(mix_lambda)
    q_all = small(queries_body, ((3072, 128), BF), 0, q_other, q_own)
    q_all, lam_got = after((q_all, lam_got))

    one = [(0, 0, 384), (0, 768, 1152)]
    two = one + [(1, 0, 384), (1, 768, 1152)]
    states = attend(q_all, [block], one, None)
    states, right, left = after((states, right, left))
    right2, left2 = around(right, 1), around(left, -1)
    states = attend(q_all, [right, left], two, states)
    states, right2, left2 = after((states, right2, left2))
    right3, left3 = around(right2, 1), around(left2, -1)
    states, from_left, from_right, carry_c = after((states, from_left, from_right, carry_c))
    far = around(from_left, 1, "x", X)
    left_c, right_c = swap(from_left), swap(from_right)
    states = attend(q_all, [right2, left2], two, states)
    states, right3, left3 = after((states, right3, left3))
    last_r, last_l = around(right3[:768], 1), around(left3[768:], -1)
    states = attend(q_all, [right3, left3], two, states)
    states, last_r, last_l, left_c, right_c = after((states, last_r, last_l, left_c, right_c))
    ends = [(0, 0, 384), (1, 0, 384)]
    (theirs,) = attend(q_all, [last_r, last_l], ends, states[:1], 1)
    other = swap(theirs)
    (own,) = attend(q_all, [last_r, last_l], ends, states[1:], 1, 6)
    own, far = after((own, far))
    far_c = swap(far)

    attended = finish(y, core, mix_lambda, lam_got, own, other, head_gain.reshape(1, 128)).reshape(Y * X, 192, 128)
    spread = exchange(attended, ("y", "x")).reshape(Y, X, 192, 128)
    blocks = [carry, carry_c, from_left, left_c, from_right, right_c, far, far_c]
    spread, weights = after((spread, weights))
    *mixed, base = layer(x, core, spread, norm_gain.reshape(1, 2048), blocks, weights)
    mixed = [around(m, step, "x", X) for m, step in zip(mixed, (2, 1, -1))]
    base, total = after((base, sum(m.astype(F32) for m in mixed)))
    return (base + 0.5 * total).astype(BF)


def solution(mesh):
    split = Mesh(mesh.devices.reshape(Z, Y, X, C), ("z", "y", "x", "c"))
    sp, tp = ("z", "y"), ("x", "c")
    return jax.shard_map(
        inner,
        mesh=split,
        in_specs=(
            P(("z", "y", "x", "c"), None),
            P(sp, tp),
            P(sp, tp),
            P(sp, tp),
            P(tp),
            P(),
            P(tp, None),
            P(),
            P(sp, tp),
            P(sp, tp),
            P(tp, sp),
        ),
        out_specs=P(("z", "y", "x", "c"), None),
        check_vma=False,
    )
```
